32 devices in a mesh: sp: 4 (over z), fs: 4 (over y, x), tp: 2 (over core).
Axes of the slice: x: 2, y: 2, z: 4, core: 2. Of those that a mesh axis runs over, the one named last changes fastest.
Arguments:
- tokens: bfloat16 [4, 512, 2048], P('fs', ('sp', 'tp')), may hold values from -6 to 6
- norm_gain: float32 [2048], replicated, may hold values from 0.1 to 1.9
- rec_query: bfloat16 [2048, 512], P('sp', 'tp'), may hold values from -0.125 to 0.125
- rec_input: bfloat16 [2048, 512], P('sp', 'tp'), may hold values from -0.125 to 0.125
- rec_forward: bfloat16 [2048, 512], P('sp', 'tp'), may hold values from -0.125 to 0.125
- rec_backward: bfloat16 [2048, 512], P('sp', 'tp'), may hold values from -0.125 to 0.125
- forget_gap: float32 [2, 512], P(None, 'tp'), may hold values from 0 to 0.06
- log_decay: float32 [4, 2, 4, 512], P('fs', None, 'tp', 'sp'), may hold values from -0.7 to 0
- rec_gain: float32 [512], P('tp'), may hold values from 0.1 to 1.9
- conv_value: bfloat16 [2048, 512], P('sp', 'tp'), may hold values from -0.125 to 0.125
- conv_gate: bfloat16 [2048, 512], P('sp', 'tp'), may hold values from -0.125 to 0.125
- conv_kernel: bfloat16 [31, 512], P(None, 'tp'), may hold values from -3.1 to 3.1
- conv_gain: float32 [512], P('tp'), may hold values from 0.1 to 1.9
- out_rec: bfloat16 [512, 2048], P('tp', 'sp'), may hold values from -0.1875 to 0.1875
- out_conv: bfloat16 [512, 2048], P('tp', 'sp'), may hold values from -0.1875 to 0.1875
Outputs:
- mixed: bfloat16 [4, 512, 2048], P('fs', ('sp', 'tp'))
The draws below stay inside these ranges and needn't reach their ends.
All inputs are finite; a program needn't handle non-finite values.
Results may differ from the reference program's by a relative error of at most 0.017.
Values may be sent and summed in bfloat16 or wider, within the bound.
A program may use at most 64 MiB of HBM per device.

```python
import jax
import jax.numpy as jnp
from jax import lax

D = 2048
RECURRENCE_HEADS = 4
KD = 128
VD = 128
CONV_WIDTH = 31
BLOCK = 64
TOK_DEV = 128
SEQUENCE_LENGTH = 512
SEQUENCE_COUNT = 4
GW = 512
KW = 512


def draw_forget_gap(key, part):
    rng_fast = jax.random.fold_in(key, 11)
    rng_gap = jax.random.fold_in(key, 12)
    fast_heads = jax.random.randint(rng_fast, (2, RECURRENCE_HEADS, 1), 0, 2) == 0
    spread = jax.random.uniform(rng_gap, (2, RECURRENCE_HEADS, KD), jnp.float32)
    fast_gap = 0.02 * jnp.power(3.0, spread)
    slow_gap = 0.2 * jnp.power(5.0, spread) / SEQUENCE_LENGTH
    chosen = jnp.where(fast_heads, fast_gap, slow_gap)
    return chosen.reshape(2, RECURRENCE_HEADS * KD).astype(jnp.float32)


def draw_log_decay(key, part):
    rng_rate = jax.random.fold_in(key, 21)
    random_spike_key = jax.random.fold_in(key, 22)
    random_length_key = jax.random.fold_in(key, 23)
    segments = SEQUENCE_LENGTH // TOK_DEV
    spread = jax.random.uniform(rng_rate, (SEQUENCE_COUNT, 2, RECURRENCE_HEADS, segments, 1), jnp.float32)
    spike_probability = 0.1 * jnp.power(10.0, spread) / SEQUENCE_LENGTH
    spike_probability = jnp.broadcast_to(spike_probability, (SEQUENCE_COUNT, 2, RECURRENCE_HEADS, segments, TOK_DEV)).reshape(SEQUENCE_COUNT, 2, RECURRENCE_HEADS, SEQUENCE_LENGTH)
    spike_active = jax.random.randint(random_spike_key, (SEQUENCE_COUNT, 2, RECURRENCE_HEADS, SEQUENCE_LENGTH), 0, SEQUENCE_LENGTH) < 2
    spike_length = jax.random.uniform(random_length_key, (SEQUENCE_COUNT, 2, RECURRENCE_HEADS, SEQUENCE_LENGTH), jnp.float32, 0.22, 0.69)
    return -(spike_probability + jnp.where(spike_active, spike_length, 0.0)).astype(jnp.float32)


def draw_conv_kernel(key, part):
    rng_base = jax.random.fold_in(key, 31)
    rng_scale = jax.random.fold_in(key, 32)
    channel_pos = jnp.arange(GW, dtype=jnp.float32) / max(GW - 1, 1)
    wobble = jax.random.uniform(rng_scale, (GW,), jnp.float32, jnp.log(0.7), jnp.log(1.4))
    channel_scale = jnp.exp(jnp.log(3.0) * channel_pos + wobble)
    base_draw = jnp.clip(jax.random.normal(rng_base, (CONV_WIDTH, GW), jnp.float32), -4.0, 4.0)
    return (base_draw * channel_scale[None, :] / jnp.sqrt(CONV_WIDTH * 1.0)).astype(jnp.bfloat16)


def block_levels(own_key, shape, split, least, largest):
    def one(dim, blocks):
        steps = jax.random.uniform(jax.random.fold_in(jax.random.fold_in(own_key, 6), dim), (blocks,), jnp.float32, least / len(split), largest / len(split))
        return jnp.repeat(jnp.exp(steps), shape[dim] // blocks).reshape((-1,) + (1,) * (len(shape) - dim - 1))

    gain = one(*split[0])
    for cut in split[1:]:
        gain = gain * one(*cut)
    return gain


def scatter_about(stream_key, dims, deviation, limit, cuts=(), kind=jnp.bfloat16):
    drawn = jax.random.normal(stream_key, dims, jnp.float32) * deviation
    if len(cuts) > 0:
        drawn = block_levels(stream_key, dims, cuts, -0.22, 0.18) * drawn
    return jnp.clip(drawn, min=-limit, max=limit).astype(kind)


def setup_inputs(seed: int = 0) -> dict:
    splits = jax.random.split(jax.random.key(seed), 16)
    return {
        "tokens": scatter_about(splits[0], (SEQUENCE_COUNT, SEQUENCE_LENGTH, D), 1.0, 6.0, ((0, 4), (1, 8))),
        "norm_gain": jnp.clip(1.0 + 0.18 * jax.random.normal(splits[1], (D,), jnp.float32), 0.1, 1.9),
        "rec_query": scatter_about(splits[2], (D, KW), D ** -0.5, 0.125, ((0, 4), (1, 2))),
        "rec_input": scatter_about(splits[3], (D, GW), D ** -0.5, 0.125, ((0, 4), (1, 2))),
        "rec_forward": scatter_about(splits[4], (D, KW), D ** -0.5, 0.125, ((0, 4), (1, 2))),
        "rec_backward": scatter_about(splits[5], (D, KW), D ** -0.5, 0.125, ((0, 4), (1, 2))),
        "forget_gap": draw_forget_gap(jax.random.fold_in(splits[15], 71), 0),
        "log_decay": draw_log_decay(jax.random.fold_in(splits[15], 71), 0),
        "rec_gain": jnp.clip(1.0 + 0.18 * jax.random.normal(splits[8], (GW,), jnp.float32), 0.1, 1.9),
        "conv_value": scatter_about(splits[9], (D, GW), D ** -0.5, 0.125, ((0, 4), (1, 2))),
        "conv_gate": scatter_about(splits[10], (D, GW), D ** -0.5, 0.125, ((0, 4), (1, 2))),
        "conv_kernel": draw_conv_kernel(jax.random.fold_in(splits[15], 71), 0),
        "conv_gain": jnp.clip(1.0 + 0.18 * jax.random.normal(splits[12], (GW,), jnp.float32), 0.1, 1.9),
        "out_rec": scatter_about(splits[13], (GW, D), (2 * GW) ** -0.5, 0.1875, ((0, 2), (1, 4))),
        "out_conv": scatter_about(splits[14], (GW, D), (2 * GW) ** -0.5, 0.1875, ((0, 2), (1, 4))),
    }


EPS = 1e-06
HIGH = lax.Precision.HIGHEST

def block_scan(queries, key_rows, value_rows, log_gate):
    heads_n, length_n, key_dim = queries.shape
    value_dim = value_rows.shape[-1]
    blocks = length_n // BLOCK

    def split_blocks(tensor):
        return tensor.reshape(heads_n, blocks, BLOCK, tensor.shape[-1]).transpose(1, 0, 2, 3)
    lower_mask = jnp.tril(jnp.ones((BLOCK, BLOCK), bool))

    def advance(states, inputs):
        query_b, key_b, value_b, gate_b = inputs
        cumulative = jnp.cumsum(gate_b, axis=1)
        query_g = query_b * jnp.exp(cumulative)
        key_g = key_b * jnp.exp(-cumulative)
        scores = jnp.einsum('htd,hsd->hts', query_g, key_g, precision=HIGH)
        scores = jnp.where(lower_mask, scores, 0.0)
        result = jnp.einsum('hts,hse->hte', scores, value_b, precision=HIGH)
        result = result + jnp.einsum('htd,hde->hte', query_g, states, precision=HIGH)
        last_g = cumulative[:, -1, :]
        weighted = key_b * jnp.exp(last_g[:, None, :] - cumulative)
        states = jnp.exp(last_g)[:, :, None] * states + jnp.einsum('hsd,hse->hde', weighted, value_b, precision=HIGH)
        return (states, result)
    start_state = jnp.zeros((heads_n, key_dim, value_dim), jnp.float32)
    inputs = (split_blocks(queries), split_blocks(key_rows), split_blocks(value_rows), split_blocks(log_gate))
    final_state, results = lax.scan(advance, start_state, inputs)
    return results.transpose(1, 0, 2, 3).reshape(heads_n, length_n, value_dim)

def to_heads(tensor):
    return tensor.astype(jnp.float32).reshape(tensor.shape[0], RECURRENCE_HEADS, -1).transpose(1, 0, 2)

def gate_terms(pre_act, gap_row, decay_row):
    closing = jax.nn.sigmoid(-to_heads(pre_act)) * gap_row.reshape(RECURRENCE_HEADS, 1, -1)
    return (closing, jnp.log1p(-closing) + decay_row[:, :, None])

def reference(tokens, norm_gain, rec_query, rec_input, rec_forward, rec_backward, forget_gap, log_decay, rec_gain, conv_value, conv_gate, conv_kernel, conv_gain, out_rec, out_conv):

    def one_sequence(inputs):
        rows_in, decay_in = inputs
        row_values = rows_in.astype(jnp.float32)
        normed = row_values * lax.rsqrt(lax.optimization_barrier(jnp.mean(row_values * row_values, axis=-1, keepdims=True)) + EPS)
        normed = (normed * norm_gain).astype(jnp.bfloat16)

        def project(weight):
            return jnp.dot(normed, weight, preferred_element_type=jnp.float32).astype(jnp.bfloat16)
        queries = jax.nn.silu(to_heads(project(rec_query))) * KD ** (-0.5)
        values = to_heads(project(rec_input))
        keys_fwd, gate_fwd = gate_terms(project(rec_forward), forget_gap[0], decay_in[0])
        keys_bwd, gate_bwd = gate_terms(project(rec_backward), forget_gap[1], decay_in[1])
        forward = block_scan(queries, keys_fwd, values, gate_fwd)
        backward = jnp.flip(block_scan(jnp.flip(queries, 1), jnp.flip(keys_bwd, 1), jnp.flip(values, 1), jnp.flip(gate_bwd, 1)), 1)
        joined = forward + backward
        joined = joined * lax.rsqrt(lax.optimization_barrier(jnp.mean(joined * joined, axis=-1, keepdims=True)) + EPS)
        joined = joined * rec_gain.reshape(RECURRENCE_HEADS, 1, VD)
        rec_out = joined.transpose(1, 0, 2).reshape(SEQUENCE_LENGTH, GW).astype(jnp.bfloat16)
        conv_pre = project(conv_value).astype(jnp.float32)
        glu_pre = project(conv_gate).astype(jnp.float32)
        gated = (conv_pre * jax.nn.sigmoid(glu_pre)).astype(jnp.bfloat16)
        convolved = lax.conv_general_dilated(gated.astype(jnp.float32)[None], conv_kernel.astype(jnp.float32)[:, None, :], (1,), 'SAME', dimension_numbers=('NWC', 'WIO', 'NWC'), feature_group_count=GW, precision=HIGH)[0]
        mean_c = lax.optimization_barrier(jnp.sum(convolved, axis=-1, keepdims=True)) / GW
        variance = lax.optimization_barrier(jnp.sum(convolved * convolved, axis=-1, keepdims=True)) / GW - mean_c * mean_c
        conv_out = jax.nn.silu((convolved - mean_c) * lax.rsqrt(variance + EPS) * conv_gain).astype(jnp.bfloat16)
        mixed = jnp.dot(rec_out, out_rec, preferred_element_type=jnp.float32)
        mixed = mixed + jnp.dot(conv_out, out_conv, preferred_element_type=jnp.float32)
        return mixed.astype(jnp.bfloat16)
    return lax.map(one_sequence, (tokens, log_decay))
```

```python
import functools

import jax
import jax.numpy as jnp
from jax import lax
from jax.experimental import pallas as pl
from jax.experimental.pallas import tpu as pltpu
from jax.sharding import PartitionSpec as P

KD = 128
VD = 128
BLOCK = 64


EPS = 1e-06
HIGH = lax.Precision.HIGHEST


def entering(x, axis, join, neutral, backward):
    count = lax.axis_size(axis)
    place = lax.axis_index(axis)
    ahead = count - 1 - place if backward else place
    gathered = jax.tree.map(
        lambda a, kind: lax.all_gather(a.astype(kind), axis), x, (jnp.bfloat16, jnp.bfloat16)
    )
    state = jax.tree.map(lambda a, e: jnp.zeros_like(a) + jnp.asarray(e, a.dtype), x, neutral)

    def one(lap, state):
        source = count - 1 - lap if backward else lap
        return join(
            state,
            jax.tree.map(
                lambda a, own: lax.dynamic_index_in_dim(a, source, 0, False).astype(own.dtype),
                gathered,
                x,
            ),
        )

    return lax.fori_loop(0, ahead, one, state)


def padded_2(cells, sides, width):
    for axis, dim in sides:
        count = lax.axis_size(axis)
        ends = count - 1
        head = lax.slice_in_dim(cells, 0, width, axis=dim)
        tail = lax.slice_in_dim(cells, cells.shape[dim] - width, cells.shape[dim], axis=dim)
        cells = jnp.concatenate(
            [
                lax.ppermute(tail, axis, [(i, (i + 1) % count) for i in range(ends)]),
                cells,
                lax.ppermute(head, axis, [((i + 1) % count, i) for i in range(ends)]),
            ],
            axis=dim,
        )
    return cells


def block_pass(queries, key_rows, value_rows, log_gate):
    heads_n, length_n, key_dim = queries.shape
    value_dim = value_rows.shape[-1]
    blocks = length_n // BLOCK

    def split_blocks(tensor):
        return tensor.reshape(heads_n, blocks, BLOCK, tensor.shape[-1]).transpose(1, 0, 2, 3)

    def join_blocks(tensor):
        return tensor.transpose(1, 0, 2, 3).reshape(heads_n, length_n, tensor.shape[-1])

    lower_mask = jnp.tril(jnp.ones((BLOCK, BLOCK), bool))

    def advance(carried, inputs):
        states, offset = carried
        query_b, key_b, value_b, gate_b = inputs
        cumulative = jnp.cumsum(gate_b, axis=1)
        query_g = query_b * jnp.exp(cumulative)
        key_g = key_b * jnp.exp(-cumulative)
        scores = jnp.einsum("htd,hsd->hts", query_g, key_g, precision=HIGH)
        scores = jnp.where(lower_mask, scores, 0.0)
        result = jnp.einsum("hts,hse->hte", scores, value_b, precision=HIGH)
        result = result + jnp.einsum("htd,hde->hte", query_g, states, precision=HIGH)
        last_g = cumulative[:, -1, :]
        weighted = key_b * jnp.exp(last_g[:, None, :] - cumulative)
        states = jnp.exp(last_g)[:, :, None] * states + jnp.einsum(
            "hsd,hse->hde", weighted, value_b, precision=HIGH
        )
        decayed = query_b * jnp.exp(offset[:, None, :] + cumulative)
        return ((states, offset + last_g), (result, decayed))

    start_state = jnp.zeros((heads_n, key_dim, value_dim), jnp.float32)
    start_offset = jnp.zeros((heads_n, key_dim), jnp.float32)
    inputs = (
        split_blocks(queries),
        split_blocks(key_rows),
        split_blocks(value_rows),
        split_blocks(log_gate),
    )
    final_pair, outputs = lax.scan(advance, (start_state, start_offset), inputs)
    return (join_blocks(outputs[0]), join_blocks(outputs[1]), final_pair[1], final_pair[0])


def chain_combine(first_part, second_part):
    return (
        first_part[0] * second_part[0],
        second_part[0][:, :, None] * first_part[1] + second_part[1],
    )


def recurrence(query_pre, input_pre, forward_pre, backward_pre, forget_gap, log_decay, rec_gain):
    heads_local = log_decay.shape[2]
    row_count = query_pre.shape[0]

    def to_heads(tensor):
        return tensor.astype(jnp.float32).reshape(row_count, heads_local, -1).transpose(1, 0, 2)

    def gate_terms(pre_act, gap_row, decay_row):
        closing = jax.nn.sigmoid(-to_heads(pre_act)) * gap_row.reshape(heads_local, 1, -1)
        return (closing, jnp.log1p(-closing) + decay_row[:, :, None])

    queries = jax.nn.silu(to_heads(query_pre)) * KD ** (-0.5)
    values = to_heads(input_pre)
    keys_fwd, gate_fwd = gate_terms(forward_pre, forget_gap[0], log_decay[0, 0])
    keys_bwd, gate_bwd = gate_terms(backward_pre, forget_gap[1], log_decay[0, 1])
    identity = (
        jnp.ones((heads_local, KD), jnp.float32),
        jnp.zeros((heads_local, KD, VD), jnp.float32),
    )
    local_fwd, decayed_fwd, offset_fwd, state_fwd = block_pass(queries, keys_fwd, values, gate_fwd)
    incoming_fwd = entering((jnp.exp(offset_fwd), state_fwd), "sp", chain_combine, identity, False)
    forward = local_fwd + jnp.einsum("htd,hde->hte", decayed_fwd, incoming_fwd[1], precision=HIGH)
    local_bwd, decayed_bwd, offset_bwd, state_bwd = block_pass(
        jnp.flip(queries, 1), jnp.flip(keys_bwd, 1), jnp.flip(values, 1), jnp.flip(gate_bwd, 1)
    )
    incoming_bwd = entering((jnp.exp(offset_bwd), state_bwd), "sp", chain_combine, identity, True)
    backward = jnp.flip(
        local_bwd + jnp.einsum("htd,hde->hte", decayed_bwd, incoming_bwd[1], precision=HIGH), 1
    )
    joined = forward + backward
    joined = joined * lax.rsqrt(jnp.mean(joined * joined, axis=-1, keepdims=True) + EPS)
    joined = joined * rec_gain.reshape(heads_local, 1, VD)
    return joined.transpose(1, 0, 2).reshape(row_count, heads_local * VD).astype(jnp.bfloat16)


def convolve(conv_pre, glu_pre, conv_kernel, conv_gain):
    gated = (conv_pre.astype(jnp.float32) * jax.nn.sigmoid(glu_pre.astype(jnp.float32))).astype(
        jnp.bfloat16
    )
    half_width = conv_kernel.shape[0] // 2
    padded = padded_2(gated, (("sp", 0),), half_width)
    convolved = lax.conv_general_dilated(
        padded.astype(jnp.float32)[None],
        conv_kernel.astype(jnp.float32)[:, None, :],
        (1,),
        "VALID",
        dimension_numbers=("NWC", "WIO", "NWC"),
        feature_group_count=gated.shape[1],
        precision=HIGH,
    )[0]
    totals = lax.psum((jnp.sum(convolved, axis=-1), jnp.sum(convolved * convolved, axis=-1)), "tp")
    full_width = convolved.shape[1] * lax.axis_size("tp")
    mean_c = (totals[0] / full_width)[:, None]
    variance = (totals[1] / full_width)[:, None] - mean_c * mean_c
    return jax.nn.silu((convolved - mean_c) * lax.rsqrt(variance + EPS) * conv_gain).astype(
        jnp.bfloat16
    )


def body(
    tokens,
    norm_gain,
    rec_query,
    rec_input,
    rec_forward,
    rec_backward,
    forget_gap,
    log_decay,
    rec_gain,
    conv_value,
    conv_gate,
    conv_kernel,
    conv_gain,
    out_rec,
    out_conv,
):
    row_values = tokens[0].astype(jnp.float32)
    normed = row_values * lax.rsqrt(jnp.mean(row_values * row_values, axis=-1, keepdims=True) + EPS)
    normed = (normed * norm_gain).astype(jnp.bfloat16)
    whole = lax.all_gather(normed, "tp", axis=0, tiled=True)
    row_count = whole.shape[0]
    pieces = (
        lax.all_gather(rec_query, "sp", axis=0, tiled=True),
        lax.all_gather(rec_input, "sp", axis=0, tiled=True),
        lax.all_gather(rec_forward, "sp", axis=0, tiled=True),
        lax.all_gather(rec_backward, "sp", axis=0, tiled=True),
        lax.all_gather(conv_value, "sp", axis=0, tiled=True),
        lax.all_gather(conv_gate, "sp", axis=0, tiled=True),
    )
    results = tuple(
        (
            jnp.dot(whole, weight_piece, preferred_element_type=jnp.float32)
            for weight_piece in pieces
        )
    )
    projected = tuple((result.astype(jnp.bfloat16) for result in results))
    rec_out = recurrence(
        projected[0], projected[1], projected[2], projected[3], forget_gap, log_decay, rec_gain
    )
    conv_out = convolve(projected[4], projected[5], conv_kernel, conv_gain)
    both_out = jnp.concatenate([rec_out, conv_out], axis=1)
    out_local = jnp.concatenate([out_rec, out_conv], axis=0)
    full_columns = lax.all_gather(out_local, "sp", axis=1, tiled=True)
    own_rows = row_count // lax.axis_size("tp")
    rows_part = lax.slice_in_dim(both_out, 0, own_rows * lax.axis_size("tp"), axis=0)
    mixed = lax.psum_scatter(
        jnp.dot(rows_part, full_columns, preferred_element_type=jnp.float32).astype(jnp.bfloat16),
        "tp",
        scatter_dimension=0,
        tiled=True,
    )
    return mixed[None]


MESH = pl.DeviceIdType.MESH
PACK = 8


def dot_as(a, b, ca, cb, precision=HIGH):
    return lax.dot_general(
        a, b, (((ca,), (cb,)), ((), ())), precision=precision, preferred_element_type=jnp.float32
    )


def fused_kernel(
    n, nf, hl, tokens, gain, w0, w1, w2, w3, w4, w5, pack, out_r, out_c, o_ref,
    x, wbuf, ow, pk, ld, dec, proj, accf, accb, gp, yout, yall, mo, fin, st,
    w_send, w_recv, x_send, x_recv, t_send, t_recv, d_send, p_send, p_recv, l_send, l_recv,
    o_send, o_recv, a_send, a_recv, f_send, f_recv, s_send, s_recv, loc,
):
    s = lax.axis_index("sp")
    f = lax.axis_index("fs")
    t = lax.axis_index("tp")
    other = 1 - t
    rows = tokens.shape[1]
    width = KD
    weights = (w0, w1, w2, w3, w4, w5)
    kslice = w0.shape[0]
    krows = kslice // nf
    half = out_r.shape[0]
    groups = n * width

    def at(sp=s, fs=f, tp=t):
        return {"sp": sp, "fs": fs, "tp": tp}

    def remote(src, dst, send, recv, to):
        return pltpu.make_async_remote_copy(
            src_ref=src, dst_ref=dst, send_sem=send, recv_sem=recv, device_id=to,
            device_id_type=MESH,
        )

    barrier = pltpu.get_barrier_semaphore()
    for d in range(n):
        for c in range(2):
            if d or c:
                pl.semaphore_signal(
                    barrier, inc=1, device_id=at(sp=lax.rem(s + d, n), tp=lax.rem(t + c, 2)),
                    device_id_type=MESH,
                )
    for d in range(1, nf):
        pl.semaphore_signal(
            barrier, inc=1, device_id=at(fs=lax.rem(f + d, nf)), device_id_type=MESH
        )
    pl.semaphore_wait(barrier, 2 * n - 1 + nf - 1)

    def wrows(place, quarter):
        return pl.ds(pl.multiple_of(place * kslice + quarter * krows, krows), krows)

    def wcols(core):
        return pl.ds(0, (4 - 2 * core) * width)

    mine = pl.ds(pl.multiple_of(f * krows, krows), krows)
    for j in range(hl):
        to_s = t * hl + j
        cols = pl.ds(j * width, width)
        for core in range(2):
            here = (to_s == s) & (t == core)
            for at_m, m in enumerate((0, 1, 2, 3) if core == 0 else (4, 5)):
                src = weights[m].at[mine, cols]
                dst = wbuf.at[wrows(s, f), pl.ds(at_m * width, width)]

                @pl.when(here)
                def _(src=src, dst=dst):
                    pltpu.make_async_copy(src, dst, w_recv.at[s]).start()

                @pl.when(jnp.logical_not(here))
                def _(src=src, dst=dst, core=core, to_s=to_s):
                    remote(
                        src, dst, w_send.at[j, core], w_recv.at[s], at(sp=to_s, tp=core)
                    ).start()

        here0 = (to_s == s) & (t == 0)
        src = pack.at[j, pl.ds(0, PACK)]

        @pl.when(here0)
        def _(src=src):
            pltpu.make_async_copy(src, ld.at[s], l_recv.at[s]).start()

        @pl.when(jnp.logical_not(here0))
        def _(src=src, j=j, to_s=to_s):
            remote(src, ld.at[s], l_send.at[j], l_recv.at[s], at(sp=to_s, tp=0)).start()

        @pl.when(to_s == s)
        def _(j=j):
            pltpu.make_async_copy(pack.at[j], pk, p_recv).start()
            remote(pack.at[j], pk, p_send, p_recv, at(tp=other)).start()

    values = tokens[0].astype(jnp.float32)
    normed = values * lax.rsqrt(jnp.mean(values * values, axis=-1, keepdims=True) + EPS)

    def slot(place, core):
        return pl.ds(pl.multiple_of(place * 2 * rows + core * rows, rows), rows)

    x[slot(s, t), :] = (normed * gain[...]).astype(jnp.bfloat16)

    def token(place, core, send, to):
        part = x.at[slot(place, core)]
        return remote(part, part, send, t_recv.at[place, core], to)

    def token_right(place):
        return token(place, t, t_send.at[place, 0], at(sp=lax.rem(s + 1, n)))

    def token_left(place):
        return token(place, t, t_send.at[place, 1], at(sp=lax.rem(s + n - 1, n)))

    def token_partner(place):
        return token(place, t, d_send.at[place], at(tp=other))

    @pl.when(s < n - 1)
    def _():
        token_right(s).start()

    @pl.when(s > 0)
    def _():
        token_left(s).start()

    token_partner(s).start()

    own_out = []
    for which, ref in enumerate((out_r, out_c)):
        part = ow.at[pl.ds(pl.multiple_of(which * groups + t * half, half), half)]
        own_out.append(remote(ref, part, o_send.at[which], o_recv.at[which], at(tp=other)))
        own_out[-1].start()
        pltpu.make_async_copy(ref, part, loc.at[which]).start()

    def share(core, place, d):
        part = wbuf.at[wrows(place, f), wcols(core)]
        return remote(
            part, part, x_send.at[place, d], x_recv.at[place, f], at(fs=lax.rem(f + d, nf))
        )

    for core in range(2):

        @pl.when(t == core)
        def _(core=core):
            for place in range(n):
                part = wbuf.at[wrows(place, f), wcols(core)]
                pltpu.make_async_copy(part, part, w_recv.at[place]).wait()
                for d in range(1, nf):
                    share(core, place, d).start()

    for d in range(1, n):

        @pl.when(s >= d)
        def _(d=d):
            place = s - d
            token_right(place).wait_recv()
            token_partner(place).start()

            @pl.when(s < n - 1)
            def _():
                token_right(place).start()

        @pl.when(s + d < n)
        def _(d=d):
            place = s + d
            token_left(place).wait_recv()
            token_partner(place).start()

            @pl.when(s > 0)
            def _():
                token_left(place).start()

    for place in range(n):
        part = x.at[slot(place, other)]
        remote(part, part, d_send.at[place], t_recv.at[place, other], at(tp=other)).wait_recv()
    for core in range(2):

        @pl.when(t == core)
        def _(core=core):
            for place in range(n):
                for d in range(1, nf):
                    quarter = lax.rem(f + d, nf)
                    part = wbuf.at[wrows(place, quarter), wcols(core)]
                    remote(
                        part, part, x_send.at[place, d], x_recv.at[place, quarter], at(fs=quarter)
                    ).wait_recv()

    pltpu.make_async_copy(pk, pk, p_recv).wait()

    total = x.shape[0]
    chunk = min(256, total)

    def project(core):
        @pl.loop(0, total // chunk)
        def _(i):
            at_rows = pl.ds(pl.multiple_of(i * chunk, chunk), chunk)
            proj[at_rows, wcols(core)] = jnp.dot(
                x[at_rows, :], wbuf[:, wcols(core)], preferred_element_type=jnp.float32
            ).astype(jnp.bfloat16)

    def send_all(core, to_s, to_t):
        dst = yall.at[:, pl.ds(pl.multiple_of(core * groups + s * width, width), width)]
        return remote(
            yout.at[to_t], dst, a_send.at[to_s, to_t], a_recv.at[s, core], at(sp=to_s, tp=to_t)
        )

    def spread(core):
        for d in range(n):
            for c in range(2):
                if d or c:
                    send_all(core, lax.rem(s + n - d, n), (core + c) % 2).start()
        dst = yall.at[:, pl.ds(pl.multiple_of(core * groups + s * width, width), width)]
        pltpu.make_async_copy(yout.at[core], dst, a_recv.at[s, core]).start()

    def spread_wait(core):
        for d in range(n):
            for c in range(2):
                if d or c:
                    send_all(core, lax.rem(s + n - d, n), (core + c) % 2).wait_send()

    @pl.when(t == 0)
    def _():
        project(0)
        for place in range(n):
            pltpu.make_async_copy(ld.at[place], ld.at[place], l_recv.at[place]).wait()
        pick = lax.broadcasted_iota(jnp.int32, (PACK, width), 0)
        span = 2 * rows
        for place in range(n):
            for d in range(2):
                dec[d, pl.ds(place * span, span), :] = dot_as(
                    ld[place], (pick == d).astype(jnp.float32), 0, 0
                )
        row_i = lax.broadcasted_iota(jnp.int32, (BLOCK, BLOCK), 0)
        col_i = lax.broadcasted_iota(jnp.int32, (BLOCK, BLOCK), 1)
        masks = (row_i >= col_i, row_i <= col_i)
        blocks = total // BLOCK

        def one(d, p, state):
            at_rows = pl.ds(pl.multiple_of(p * BLOCK, BLOCK), BLOCK)
            qp = proj[at_rows, 0:width].astype(jnp.float32)
            query = qp * jax.nn.sigmoid(qp) * width ** (-0.5)
            value = proj[at_rows, width : 2 * width].astype(jnp.float32)
            pre = proj[at_rows, (2 + d) * width : (3 + d) * width].astype(jnp.float32)
            keys = pk[2 + d : 3 + d, :] * jax.nn.sigmoid(-pre)
            gate = jnp.log1p(-keys) + dec[d, at_rows, :]
            cum = dot_as(masks[d].astype(jnp.float32), gate, 1, 0)
            query_g = query * jnp.exp(cum)
            key_g = keys * jnp.exp(-cum)
            scores = jnp.where(masks[d], dot_as(query_g, key_g, 1, 1), 0.0)
            result = dot_as(scores, value, 1, 0) + dot_as(query_g, state, 1, 1)
            last = cum[BLOCK - 1 : BLOCK, :] if d == 0 else cum[0:1, :]
            weighted = keys * jnp.exp(last - cum)
            state = state * jnp.exp(last) + dot_as(value, weighted, 0, 0)
            (accf, accb)[d][at_rows, :] = result
            return state

        def step(i, states):
            return one(0, i, states[0]), one(1, blocks - 1 - i, states[1])

        zero = jnp.zeros((width, width), jnp.float32)
        lax.fori_loop(0, blocks, step, (zero, zero))
        for place in range(n):
            for c in range(2):
                at_rows = pl.ds((place * 2 + c) * rows, rows)
                joined = accf[at_rows, :] + accb[at_rows, :]
                joined = joined * lax.rsqrt(
                    jnp.mean(joined * joined, axis=-1, keepdims=True) + EPS
                )
                yout[c, pl.ds(place * rows, rows), :] = (joined * pk[4:5, :]).astype(jnp.bfloat16)
        spread(0)

    @pl.when(t == 1)
    def _():
        project(1)
        taps = pk.shape[0] - PACK
        pad = 16
        gp[0:pad, :] = jnp.zeros((pad, width), jnp.float32)
        gp[pad + total : 2 * pad + total, :] = jnp.zeros((pad, width), jnp.float32)
        value = proj[:, 0:width].astype(jnp.float32)
        gate = proj[:, width : 2 * width].astype(jnp.float32)
        gp[pad : pad + total, :] = (
            (value * jax.nn.sigmoid(gate)).astype(jnp.bfloat16).astype(jnp.float32)
        )
        first = pad - taps_half(taps)

        for b in range(total // rows):
            acc = jnp.zeros((rows, width), jnp.float32)
            for j in range(taps):
                acc = acc + pk[PACK + j : PACK + j + 1, :] * gp[pl.ds(b * rows + first + j, rows), :]
            accf[pl.ds(b * rows, rows), :] = acc
        conv = accf[...]
        ones = jnp.ones((8, width), jnp.float32)
        st[s, 0] = dot_as(ones, conv, 1, 1)
        st[s, 1] = dot_as(ones, conv * conv, 1, 1)

        def stat(d):
            return remote(
                st.at[s], st.at[s], s_send.at[d], s_recv.at[s], at(sp=lax.rem(s + d, n))
            )

        for d in range(1, n):
            stat(d).start()
        for d in range(1, n):
            place = lax.rem(s + d, n)
            remote(st.at[place], st.at[place], s_send.at[d], s_recv.at[place], at(sp=place)).wait_recv()
        stats = st[0]
        for place in range(1, n):
            stats = stats + st[place]
        stats = stats / groups
        mean_r = stats[0]
        inv_r = lax.rsqrt(stats[1] - mean_r * mean_r + EPS)
        eighth = jnp.full((8, width), 0.125, jnp.float32)
        mean_c = dot_as(mean_r, eighth, 0, 0)
        inv_c = dot_as(inv_r, eighth, 0, 0)
        out = (accf[...] - mean_c) * inv_c * pk[5:6, :]
        out = (out * jax.nn.sigmoid(out)).astype(jnp.bfloat16)
        for place in range(n):
            for c in range(2):
                b = (place * 2 + c) * rows
                yout[c, pl.ds(place * rows, rows), :] = out[b : b + rows]
        spread(1)
        for d in range(1, n):
            stat(d).wait_send()

    for which, ref in enumerate((out_r, out_c)):
        part = ow.at[pl.ds(pl.multiple_of(which * groups + t * half, half), half)]
        pltpu.make_async_copy(ref, part, loc.at[which]).wait()
        part = ow.at[pl.ds(pl.multiple_of(which * groups + other * half, half), half)]
        remote(ref, part, o_send.at[which], o_recv.at[which], at(tp=other)).wait_recv()
    for core in range(2):
        for place in range(n):
            part = yall.at[:, pl.ds(core * groups + place * width, width)]
            pltpu.make_async_copy(part, part, a_recv.at[place, core]).wait()
    result = jnp.dot(yall[...], ow[...], preferred_element_type=jnp.float32)
    mo[...] = result.astype(jnp.bfloat16)
    cols = out_r.shape[1]
    fin_cols = pl.ds(pl.multiple_of(s * cols, cols), cols)

    def give(to_s):
        return remote(
            mo.at[pl.ds(pl.multiple_of(to_s * rows, rows), rows)], fin.at[:, fin_cols],
            f_send.at[to_s], f_recv.at[s], at(sp=to_s),
        )

    for d in range(1, n):
        give(lax.rem(s + d, n)).start()
    o_ref[0, :, fin_cols] = mo[pl.ds(pl.multiple_of(s * rows, rows), rows), :]
    for d in range(1, n):
        place = lax.rem(s + d, n)
        part_cols = pl.ds(pl.multiple_of(place * cols, cols), cols)
        remote(
            mo.at[pl.ds(0, rows)], fin.at[:, part_cols], f_send.at[place], f_recv.at[place],
            at(sp=place),
        ).wait_recv()
        o_ref[0, :, part_cols] = fin[:, part_cols]

    for core in range(2):

        @pl.when(t == core)
        def _(core=core):
            spread_wait(core)
            for place in range(n):
                for d in range(1, nf):
                    share(core, place, d).wait_send()

    for d in range(1, n):
        give(lax.rem(s + d, n)).wait_send()
    for copy in own_out:
        copy.wait_send()
    for j in range(hl):
        to_s = t * hl + j
        for core in range(2):

            @pl.when(jnp.logical_not((to_s == s) & (t == core)))
            def _(j=j, core=core, to_s=to_s):
                part = wbuf.at[wrows(s, f), wcols(core)]
                remote(
                    part, part, w_send.at[j, core], w_recv.at[s], at(sp=to_s, tp=core)
                ).wait_send()

        @pl.when(jnp.logical_not((to_s == s) & (t == 0)))
        def _(j=j, to_s=to_s):
            remote(
                pack.at[j, pl.ds(0, PACK)], ld.at[s], l_send.at[j], l_recv.at[s],
                at(sp=to_s, tp=0),
            ).wait_send()

        @pl.when(to_s == s)
        def _(j=j):
            remote(pack.at[j], pk, p_send, p_recv, at(tp=other)).wait_send()

    for place in range(n):
        token_partner(place).wait_send()

        @pl.when((place <= s) & (s < n - 1))
        def _(place=place):
            token_right(place).wait_send()

        @pl.when((place >= s) & (s > 0))
        def _(place=place):
            token_left(place).wait_send()


def taps_half(taps):
    return taps // 2


def fused_body(
    n, nf, tokens, norm_gain, rec_query, rec_input, rec_forward, rec_backward, forget_gap,
    log_decay, rec_gain, conv_value, conv_gate, conv_kernel, conv_gain, out_rec, out_conv,
):
    hl = log_decay.shape[2]
    rows, d = tokens.shape[1:]
    total = 2 * rows * n
    taps = conv_kernel.shape[0]
    width = KD
    groups = n * width
    cols = out_rec.shape[1]

    def by_head(a):
        return a.astype(jnp.float32).reshape(-1, hl, width).transpose(1, 0, 2)

    pack = jnp.concatenate(
        [
            log_decay[0].transpose(1, 0, 2),
            by_head(forget_gap),
            by_head(rec_gain),
            by_head(conv_gain),
            jnp.zeros((hl, PACK - 6, width), jnp.float32),
            by_head(conv_kernel),
        ],
        axis=1,
    )
    vmem = pl.BlockSpec(memory_space=pltpu.VMEM)
    bf, f32 = jnp.bfloat16, jnp.float32
    dma = pltpu.SemaphoreType.DMA
    scratch = [
        pltpu.VMEM((total, d), bf),
        pltpu.VMEM((d, 4 * width), bf),
        pltpu.VMEM((2 * groups, cols), bf),
        pltpu.VMEM((PACK + taps, width), f32),
        pltpu.VMEM((n, PACK, width), f32),
        pltpu.VMEM((2, total, width), f32),
        pltpu.VMEM((total, 4 * width), bf),
        pltpu.VMEM((total, width), f32),
        pltpu.VMEM((total, width), f32),
        pltpu.VMEM((total + 32, width), f32),
        pltpu.VMEM((2, total // 2, width), bf),
        pltpu.VMEM((total // 2, 2 * groups), bf),
        pltpu.VMEM((total // 2, cols), bf),
        pltpu.VMEM((rows, d), bf),
        pltpu.VMEM((n, 2, 8, total), f32),
        dma((hl, 2)), dma((n,)),
        dma((n, nf)), dma((n, nf)),
        dma((n, 2)), dma((n, 2)), dma((n,)),
        dma(()), dma(()),
        dma((hl,)), dma((n,)),
        dma((2,)), dma((2,)),
        dma((n, 2)), dma((n, 2)),
        dma((n,)), dma((n,)),
        dma((n,)), dma((n,)),
        dma((2,)),
    ]
    return pl.pallas_call(
        functools.partial(fused_kernel, n, nf, hl),
        out_shape=jax.ShapeDtypeStruct((1, rows, d), bf),
        in_specs=[vmem] * 11,
        out_specs=vmem,
        scratch_shapes=scratch,
        compiler_params=pltpu.CompilerParams(
            collective_id=0, has_side_effects=True, vmem_limit_bytes=40 * 1024 * 1024
        ),
    )(
        tokens, norm_gain[None], rec_query, rec_input, rec_forward, rec_backward, conv_value,
        conv_gate, pack, out_rec, out_conv,
    )


def fits(n, nf, nt, tokens, rec_query, log_decay, conv_value, conv_kernel, out_rec):
    heads = log_decay.shape[2]
    rows = tokens.shape[1] // (n * nt)
    return (
        nt == 2
        and n == heads
        and tokens.shape[0] == nf
        and rec_query.shape[1] == heads * KD
        and conv_value.shape[1] == heads * VD
        and KD == VD
        and 2 * rows == KD
        and rec_query.shape[0] % (n * nf * 16) == 0
        and conv_kernel.shape[0] // 2 <= 15
    )


def layer(mesh, *args):
    n, nf, nt = (mesh.shape[a] for a in ("sp", "fs", "tp"))
    fast = fits(n, nf, nt, args[0], args[2], args[7], args[9], args[11], args[13])
    return sharded(mesh, functools.partial(fused_body, n, nf) if fast else body)(*args)


def solution(mesh):
    return functools.partial(layer, mesh)


def sharded(mesh, body):
    return jax.shard_map(
        body,
        mesh=mesh,
        in_specs=(
            P("fs", ("sp", "tp"), None),
            P(),
            P("sp", "tp"),
            P("sp", "tp"),
            P("sp", "tp"),
            P("sp", "tp"),
            P(None, "tp"),
            P("fs", None, "tp", "sp"),
            P("tp"),
            P("sp", "tp"),
            P("sp", "tp"),
            P(None, "tp"),
            P("tp"),
            P("tp", "sp"),
            P("tp", "sp"),
        ),
        out_specs=P("fs", ("sp", "tp"), None),
        check_vma=False,
    )
```

```python
import functools

import jax
import jax.numpy as jnp
from jax import lax
from jax.experimental import pallas as pl
from jax.experimental.pallas import tpu as pltpu
from jax.sharding import PartitionSpec as P

KD = 128
VD = 128
BLOCK = 64


EPS = 1e-06
HIGH = lax.Precision.HIGHEST


def entering(x, axis, join, neutral, backward):
    count = lax.axis_size(axis)
    place = lax.axis_index(axis)
    ahead = count - 1 - place if backward else place
    gathered = jax.tree.map(
        lambda a, kind: lax.all_gather(a.astype(kind), axis), x, (jnp.bfloat16, jnp.bfloat16)
    )
    state = jax.tree.map(lambda a, e: jnp.zeros_like(a) + jnp.asarray(e, a.dtype), x, neutral)

    def one(lap, state):
        source = count - 1 - lap if backward else lap
        return join(
            state,
            jax.tree.map(
                lambda a, own: lax.dynamic_index_in_dim(a, source, 0, False).astype(own.dtype),
                gathered,
                x,
            ),
        )

    return lax.fori_loop(0, ahead, one, state)


def padded_2(cells, sides, width):
    for axis, dim in sides:
        count = lax.axis_size(axis)
        ends = count - 1
        head = lax.slice_in_dim(cells, 0, width, axis=dim)
        tail = lax.slice_in_dim(cells, cells.shape[dim] - width, cells.shape[dim], axis=dim)
        cells = jnp.concatenate(
            [
                lax.ppermute(tail, axis, [(i, (i + 1) % count) for i in range(ends)]),
                cells,
                lax.ppermute(head, axis, [((i + 1) % count, i) for i in range(ends)]),
            ],
            axis=dim,
        )
    return cells


def block_pass(queries, key_rows, value_rows, log_gate):
    heads_n, length_n, key_dim = queries.shape
    value_dim = value_rows.shape[-1]
    blocks = length_n // BLOCK

    def split_blocks(tensor):
        return tensor.reshape(heads_n, blocks, BLOCK, tensor.shape[-1]).transpose(1, 0, 2, 3)

    def join_blocks(tensor):
        return tensor.transpose(1, 0, 2, 3).reshape(heads_n, length_n, tensor.shape[-1])

    lower_mask = jnp.tril(jnp.ones((BLOCK, BLOCK), bool))

    def advance(carried, inputs):
        states, offset = carried
        query_b, key_b, value_b, gate_b = inputs
        cumulative = jnp.cumsum(gate_b, axis=1)
        query_g = query_b * jnp.exp(cumulative)
        key_g = key_b * jnp.exp(-cumulative)
        scores = jnp.einsum("htd,hsd->hts", query_g, key_g, precision=HIGH)
        scores = jnp.where(lower_mask, scores, 0.0)
        result = jnp.einsum("hts,hse->hte", scores, value_b, precision=HIGH)
        result = result + jnp.einsum("htd,hde->hte", query_g, states, precision=HIGH)
        last_g = cumulative[:, -1, :]
        weighted = key_b * jnp.exp(last_g[:, None, :] - cumulative)
        states = jnp.exp(last_g)[:, :, None] * states + jnp.einsum(
            "hsd,hse->hde", weighted, value_b, precision=HIGH
        )
        decayed = query_b * jnp.exp(offset[:, None, :] + cumulative)
        return ((states, offset + last_g), (result, decayed))

    start_state = jnp.zeros((heads_n, key_dim, value_dim), jnp.float32)
    start_offset = jnp.zeros((heads_n, key_dim), jnp.float32)
    inputs = (
        split_blocks(queries),
        split_blocks(key_rows),
        split_blocks(value_rows),
        split_blocks(log_gate),
    )
    final_pair, outputs = lax.scan(advance, (start_state, start_offset), inputs)
    return (join_blocks(outputs[0]), join_blocks(outputs[1]), final_pair[1], final_pair[0])


def chain_combine(first_part, second_part):
    return (
        first_part[0] * second_part[0],
        second_part[0][:, :, None] * first_part[1] + second_part[1],
    )


def recurrence(query_pre, input_pre, forward_pre, backward_pre, forget_gap, log_decay, rec_gain):
    heads_local = log_decay.shape[2]
    row_count = query_pre.shape[0]

    def to_heads(tensor):
        return tensor.astype(jnp.float32).reshape(row_count, heads_local, -1).transpose(1, 0, 2)

    def gate_terms(pre_act, gap_row, decay_row):
        closing = jax.nn.sigmoid(-to_heads(pre_act)) * gap_row.reshape(heads_local, 1, -1)
        return (closing, jnp.log1p(-closing) + decay_row[:, :, None])

    queries = jax.nn.silu(to_heads(query_pre)) * KD ** (-0.5)
    values = to_heads(input_pre)
    keys_fwd, gate_fwd = gate_terms(forward_pre, forget_gap[0], log_decay[0, 0])
    keys_bwd, gate_bwd = gate_terms(backward_pre, forget_gap[1], log_decay[0, 1])
    identity = (
        jnp.ones((heads_local, KD), jnp.float32),
        jnp.zeros((heads_local, KD, VD), jnp.float32),
    )
    local_fwd, decayed_fwd, offset_fwd, state_fwd = block_pass(queries, keys_fwd, values, gate_fwd)
    incoming_fwd = entering((jnp.exp(offset_fwd), state_fwd), "sp", chain_combine, identity, False)
    forward = local_fwd + jnp.einsum("htd,hde->hte", decayed_fwd, incoming_fwd[1], precision=HIGH)
    local_bwd, decayed_bwd, offset_bwd, state_bwd = block_pass(
        jnp.flip(queries, 1), jnp.flip(keys_bwd, 1), jnp.flip(values, 1), jnp.flip(gate_bwd, 1)
    )
    incoming_bwd = entering((jnp.exp(offset_bwd), state_bwd), "sp", chain_combine, identity, True)
    backward = jnp.flip(
        local_bwd + jnp.einsum("htd,hde->hte", decayed_bwd, incoming_bwd[1], precision=HIGH), 1
    )
    joined = forward + backward
    joined = joined * lax.rsqrt(jnp.mean(joined * joined, axis=-1, keepdims=True) + EPS)
    joined = joined * rec_gain.reshape(heads_local, 1, VD)
    return joined.transpose(1, 0, 2).reshape(row_count, heads_local * VD).astype(jnp.bfloat16)


def convolve(conv_pre, glu_pre, conv_kernel, conv_gain):
    gated = (conv_pre.astype(jnp.float32) * jax.nn.sigmoid(glu_pre.astype(jnp.float32))).astype(
        jnp.bfloat16
    )
    half_width = conv_kernel.shape[0] // 2
    padded = padded_2(gated, (("sp", 0),), half_width)
    convolved = lax.conv_general_dilated(
        padded.astype(jnp.float32)[None],
        conv_kernel.astype(jnp.float32)[:, None, :],
        (1,),
        "VALID",
        dimension_numbers=("NWC", "WIO", "NWC"),
        feature_group_count=gated.shape[1],
        precision=HIGH,
    )[0]
    totals = lax.psum((jnp.sum(convolved, axis=-1), jnp.sum(convolved * convolved, axis=-1)), "tp")
    full_width = convolved.shape[1] * lax.axis_size("tp")
    mean_c = (totals[0] / full_width)[:, None]
    variance = (totals[1] / full_width)[:, None] - mean_c * mean_c
    return jax.nn.silu((convolved - mean_c) * lax.rsqrt(variance + EPS) * conv_gain).astype(
        jnp.bfloat16
    )


def body(
    tokens,
    norm_gain,
    rec_query,
    rec_input,
    rec_forward,
    rec_backward,
    forget_gap,
    log_decay,
    rec_gain,
    conv_value,
    conv_gate,
    conv_kernel,
    conv_gain,
    out_rec,
    out_conv,
):
    row_values = tokens[0].astype(jnp.float32)
    normed = row_values * lax.rsqrt(jnp.mean(row_values * row_values, axis=-1, keepdims=True) + EPS)
    normed = (normed * norm_gain).astype(jnp.bfloat16)
    whole = lax.all_gather(normed, "tp", axis=0, tiled=True)
    row_count = whole.shape[0]
    pieces = (
        lax.all_gather(rec_query, "sp", axis=0, tiled=True),
        lax.all_gather(rec_input, "sp", axis=0, tiled=True),
        lax.all_gather(rec_forward, "sp", axis=0, tiled=True),
        lax.all_gather(rec_backward, "sp", axis=0, tiled=True),
        lax.all_gather(conv_value, "sp", axis=0, tiled=True),
        lax.all_gather(conv_gate, "sp", axis=0, tiled=True),
    )
    results = tuple(
        (
            jnp.dot(whole, weight_piece, preferred_element_type=jnp.float32)
            for weight_piece in pieces
        )
    )
    projected = tuple((result.astype(jnp.bfloat16) for result in results))
    rec_out = recurrence(
        projected[0], projected[1], projected[2], projected[3], forget_gap, log_decay, rec_gain
    )
    conv_out = convolve(projected[4], projected[5], conv_kernel, conv_gain)
    both_out = jnp.concatenate([rec_out, conv_out], axis=1)
    out_local = jnp.concatenate([out_rec, out_conv], axis=0)
    full_columns = lax.all_gather(out_local, "sp", axis=1, tiled=True)
    own_rows = row_count // lax.axis_size("tp")
    rows_part = lax.slice_in_dim(both_out, 0, own_rows * lax.axis_size("tp"), axis=0)
    mixed = lax.psum_scatter(
        jnp.dot(rows_part, full_columns, preferred_element_type=jnp.float32).astype(jnp.bfloat16),
        "tp",
        scatter_dimension=0,
        tiled=True,
    )
    return mixed[None]


MESH = pl.DeviceIdType.MESH
PACK = 8


def dot_as(a, b, ca, cb, precision=HIGH):
    return lax.dot_general(
        a, b, (((ca,), (cb,)), ((), ())), precision=precision, preferred_element_type=jnp.float32
    )


def fused_kernel(
    n, nf, hl, tokens_in, gain_in, w0, w1, w2, w3, w4, w5, decay_in, gap_in,
    rgain_in, cgain_in, taps_in, out_r, out_c, o_ref, decay_v, gap_v, rgain_v, cgain_v, taps_v,
    tokens, gain, pack,    x, wbuf, ow, pk, ld, dec, proj, accf, accb, gp, yout, yall, mo, fin, st,
    w_send, w_recv, x_send, x_recv, t_send, t_recv, d_send, p_send, p_recv, l_send, l_recv,
    o_send, o_recv, a_send, a_recv, f_send, f_recv, s_send, s_recv, loc, ini,
):
    s = lax.axis_index("sp")
    f = lax.axis_index("fs")
    t = lax.axis_index("tp")
    other = 1 - t
    rows = tokens.shape[1]
    width = KD
    weights = (w0, w1, w2, w3, w4, w5)
    kslice = w0.shape[0]
    krows = kslice // nf
    half = out_r.shape[0]
    groups = n * width

    def at(sp=s, fs=f, tp=t):
        return {"sp": sp, "fs": fs, "tp": tp}

    def remote(src, dst, send, recv, to):
        return pltpu.make_async_remote_copy(
            src_ref=src, dst_ref=dst, send_sem=send, recv_sem=recv, device_id=to,
            device_id_type=MESH,
        )

    entry = [
        pltpu.make_async_copy(src, dst, ini.at[i])
        for i, (src, dst) in enumerate(
            (
                (tokens_in, tokens), (gain_in, gain), (decay_in, decay_v), (gap_in, gap_v),
                (rgain_in, rgain_v), (cgain_in, cgain_v), (taps_in, taps_v),
            )
        )
    ]
    for copy in entry:
        copy.start()

    barrier = pltpu.get_barrier_semaphore()
    for d in range(n):
        for c in range(2):
            if d or c:
                pl.semaphore_signal(
                    barrier, inc=1, device_id=at(sp=lax.rem(s + d, n), tp=lax.rem(t + c, 2)),
                    device_id_type=MESH,
                )
    for d in range(1, nf):
        pl.semaphore_signal(
            barrier, inc=1, device_id=at(fs=lax.rem(f + d, nf)), device_id_type=MESH
        )
    pl.semaphore_wait(barrier, 2 * n - 1 + nf - 1)

    def wrows(place, quarter):
        return pl.ds(pl.multiple_of(place * kslice + quarter * krows, krows), krows)

    def wcols(core):
        return pl.ds(0, (4 - 2 * core) * width)

    def whole(place):
        return pl.ds(pl.multiple_of(place * kslice, kslice), kslice)

    mine = pl.ds(pl.multiple_of(f * krows, krows), krows)
    for j in range(hl):
        to_s = t * hl + j
        cols = pl.ds(j * width, width)
        for core in range(2):
            for at_m, m in enumerate((0, 1, 2, 3) if core == 0 else (4, 5)):
                at_cols = pl.ds(at_m * width, width)
                src = weights[m].at[:, cols]
                dst = wbuf.at[whole(s), at_cols]

                @pl.when((to_s == s) & (t == core))
                def _(src=src, dst=dst):
                    pltpu.make_async_copy(src, dst, w_recv.at[s]).start()

                @pl.when((to_s == s) & (t != core))
                def _(src=src, dst=dst, core=core, j=j):
                    remote(src, dst, w_send.at[j, core], w_recv.at[s], at(tp=core)).start()

                @pl.when(to_s != s)
                def _(m=m, cols=cols, at_cols=at_cols, core=core, to_s=to_s, j=j):
                    remote(
                        weights[m].at[mine, cols], wbuf.at[wrows(s, f), at_cols],
                        w_send.at[j, core], w_recv.at[s], at(sp=to_s, tp=core),
                    ).start()

    for copy in entry[2:]:
        copy.wait()
    taps_n = taps_v.shape[0]
    for j in range(hl):
        cols = slice(j * width, (j + 1) * width)
        pack[j, 0:2, :] = decay_v[0, :, j, :]
        pack[j, 2:4, :] = gap_v[:, cols]
        pack[j, 4:5, :] = rgain_v[:, cols]
        pack[j, 5:6, :] = cgain_v[:, cols]
        pack[j, 6:PACK, :] = jnp.zeros((PACK - 6, width), jnp.float32)
        pack[j, PACK : PACK + taps_n, :] = taps_v[:, cols].astype(jnp.float32)
    entry[0].wait()
    entry[1].wait()
    values = tokens[0].astype(jnp.float32)
    normed = values * lax.rsqrt(jnp.mean(values * values, axis=-1, keepdims=True) + EPS)

    def slot(place, core):
        return pl.ds(pl.multiple_of(place * 2 * rows + core * rows, rows), rows)

    x[slot(s, t), :] = (normed * gain[...]).astype(jnp.bfloat16)

    def token(place, core, send, to):
        part = x.at[slot(place, core)]
        return remote(part, part, send, t_recv.at[place, core], to)

    def token_right(place):
        return token(place, t, t_send.at[place, 0], at(sp=lax.rem(s + 1, n)))

    def token_left(place):
        return token(place, t, t_send.at[place, 1], at(sp=lax.rem(s + n - 1, n)))

    def token_partner(place):
        return token(place, t, d_send.at[place], at(tp=other))

    @pl.when(s < n - 1)
    def _():
        token_right(s).start()

    @pl.when(s > 0)
    def _():
        token_left(s).start()

    token_partner(s).start()

    for j in range(hl):
        to_s = t * hl + j
        here0 = (to_s == s) & (t == 0)
        src = pack.at[j, pl.ds(0, PACK)]

        @pl.when(here0)
        def _(src=src):
            pltpu.make_async_copy(src, ld.at[s], l_recv.at[s]).start()

        @pl.when(jnp.logical_not(here0))
        def _(src=src, j=j, to_s=to_s):
            remote(src, ld.at[s], l_send.at[j], l_recv.at[s], at(sp=to_s, tp=0)).start()

        @pl.when(to_s == s)
        def _(j=j):
            pltpu.make_async_copy(pack.at[j], pk, p_recv).start()
            remote(pack.at[j], pk, p_send, p_recv, at(tp=other)).start()

    own_out = []
    for which, ref in enumerate((out_r, out_c)):
        part = ow.at[pl.ds(pl.multiple_of(which * groups + t * half, half), half)]
        own_out.append(remote(ref, part, o_send.at[which], o_recv.at[which], at(tp=other)))
        own_out[-1].start()
        pltpu.make_async_copy(ref, part, loc.at[which]).start()

    def share(core, place, d):
        part = wbuf.at[wrows(place, f), wcols(core)]
        return remote(
            part, part, x_send.at[place, d], x_recv.at[place, f], at(fs=lax.rem(f + d, nf))
        )

    for core in range(2):

        @pl.when(t == core)
        def _(core=core):
            for e in range(1, n):
                place = lax.rem(s + e, n)
                part = wbuf.at[wrows(place, f), wcols(core)]
                pltpu.make_async_copy(part, part, w_recv.at[place]).wait()
                for d in range(1, nf):
                    share(core, place, d).start()

    for d in range(1, n):

        @pl.when(s >= d)
        def _(d=d):
            place = s - d
            token_right(place).wait_recv()
            token_partner(place).start()

            @pl.when(s < n - 1)
            def _():
                token_right(place).start()

        @pl.when(s + d < n)
        def _(d=d):
            place = s + d
            token_left(place).wait_recv()
            token_partner(place).start()

            @pl.when(s > 0)
            def _():
                token_left(place).start()

    for place in range(n):
        part = x.at[slot(place, other)]
        remote(part, part, d_send.at[place], t_recv.at[place, other], at(tp=other)).wait_recv()
    for core in range(2):

        @pl.when(t == core)
        def _(core=core):
            part = wbuf.at[whole(s), wcols(core)]
            pltpu.make_async_copy(part, part, w_recv.at[s]).wait()
            for e in range(1, n):
                place = lax.rem(s + e, n)
                for d in range(1, nf):
                    quarter = lax.rem(f + d, nf)
                    part = wbuf.at[wrows(place, quarter), wcols(core)]
                    remote(
                        part, part, x_send.at[place, d], x_recv.at[place, quarter], at(fs=quarter)
                    ).wait_recv()

    pltpu.make_async_copy(pk, pk, p_recv).wait()

    total = x.shape[0]
    chunk = min(256, total)

    def project(core):
        @pl.loop(0, total // chunk)
        def _(i):
            at_rows = pl.ds(pl.multiple_of(i * chunk, chunk), chunk)
            proj[at_rows, wcols(core)] = jnp.dot(
                x[at_rows, :], wbuf[:, wcols(core)], preferred_element_type=jnp.float32
            ).astype(jnp.bfloat16)

    def send_all(core, to_s, to_t):
        dst = yall.at[:, pl.ds(pl.multiple_of(core * groups + s * width, width), width)]
        return remote(
            yout.at[to_t], dst, a_send.at[to_s, to_t], a_recv.at[s, core], at(sp=to_s, tp=to_t)
        )

    def spread(core):
        for d in range(n):
            for c in range(2):
                if d or c:
                    send_all(core, lax.rem(s + n - d, n), (core + c) % 2).start()
        dst = yall.at[:, pl.ds(pl.multiple_of(core * groups + s * width, width), width)]
        pltpu.make_async_copy(yout.at[core], dst, a_recv.at[s, core]).start()

    def spread_wait(core):
        for d in range(n):
            for c in range(2):
                if d or c:
                    send_all(core, lax.rem(s + n - d, n), (core + c) % 2).wait_send()

    @pl.when(t == 0)
    def _():
        project(0)
        for place in range(n):
            pltpu.make_async_copy(ld.at[place], ld.at[place], l_recv.at[place]).wait()
        pick = lax.broadcasted_iota(jnp.int32, (PACK, width), 0)
        span = 2 * rows
        for place in range(n):
            for d in range(2):
                dec[d, pl.ds(place * span, span), :] = dot_as(
                    ld[place], (pick == d).astype(jnp.float32), 0, 0
                )
        row_i = lax.broadcasted_iota(jnp.int32, (BLOCK, BLOCK), 0)
        col_i = lax.broadcasted_iota(jnp.int32, (BLOCK, BLOCK), 1)
        masks = (row_i >= col_i, row_i <= col_i)
        blocks = total // BLOCK

        def one(d, p, state):
            at_rows = pl.ds(pl.multiple_of(p * BLOCK, BLOCK), BLOCK)
            qp = proj[at_rows, 0:width].astype(jnp.float32)
            query = qp * jax.nn.sigmoid(qp) * width ** (-0.5)
            value = proj[at_rows, width : 2 * width].astype(jnp.float32)
            pre = proj[at_rows, (2 + d) * width : (3 + d) * width].astype(jnp.float32)
            keys = pk[2 + d : 3 + d, :] * jax.nn.sigmoid(-pre)
            gate = jnp.log1p(-keys) + dec[d, at_rows, :]
            cum = dot_as(masks[d].astype(jnp.float32), gate, 1, 0)
            query_g = query * jnp.exp(cum)
            key_g = keys * jnp.exp(-cum)
            scores = jnp.where(masks[d], dot_as(query_g, key_g, 1, 1), 0.0)
            result = dot_as(scores, value, 1, 0) + dot_as(query_g, state, 1, 1)
            last = cum[BLOCK - 1 : BLOCK, :] if d == 0 else cum[0:1, :]
            weighted = keys * jnp.exp(last - cum)
            state = state * jnp.exp(last) + dot_as(value, weighted, 0, 0)
            (accf, accb)[d][at_rows, :] = result
            return state

        def step(i, states):
            return one(0, i, states[0]), one(1, blocks - 1 - i, states[1])

        zero = jnp.zeros((width, width), jnp.float32)
        lax.fori_loop(0, blocks, step, (zero, zero))
        for place in range(n):
            for c in range(2):
                at_rows = pl.ds((place * 2 + c) * rows, rows)
                joined = accf[at_rows, :] + accb[at_rows, :]
                joined = joined * lax.rsqrt(
                    jnp.mean(joined * joined, axis=-1, keepdims=True) + EPS
                )
                yout[c, pl.ds(place * rows, rows), :] = (joined * pk[4:5, :]).astype(jnp.bfloat16)
        spread(0)

    @pl.when(t == 1)
    def _():
        project(1)
        taps = pk.shape[0] - PACK
        pad = 16
        gp[0:pad, :] = jnp.zeros((pad, width), jnp.float32)
        gp[pad + total : 2 * pad + total, :] = jnp.zeros((pad, width), jnp.float32)
        value = proj[:, 0:width].astype(jnp.float32)
        gate = proj[:, width : 2 * width].astype(jnp.float32)
        gp[pad : pad + total, :] = (
            (value * jax.nn.sigmoid(gate)).astype(jnp.bfloat16).astype(jnp.float32)
        )
        first = pad - taps_half(taps)

        for b in range(total // rows):
            acc = jnp.zeros((rows, width), jnp.float32)
            for j in range(taps):
                acc = acc + pk[PACK + j : PACK + j + 1, :] * gp[pl.ds(b * rows + first + j, rows), :]
            accf[pl.ds(b * rows, rows), :] = acc
        conv = accf[...]
        ones = jnp.ones((8, width), jnp.float32)
        st[s, 0] = dot_as(ones, conv, 1, 1)
        st[s, 1] = dot_as(ones, conv * conv, 1, 1)

        def stat(d):
            return remote(
                st.at[s], st.at[s], s_send.at[d], s_recv.at[s], at(sp=lax.rem(s + d, n))
            )

        for d in range(1, n):
            stat(d).start()
        for d in range(1, n):
            place = lax.rem(s + d, n)
            remote(st.at[place], st.at[place], s_send.at[d], s_recv.at[place], at(sp=place)).wait_recv()
        stats = st[0]
        for place in range(1, n):
            stats = stats + st[place]
        stats = stats / groups
        mean_r = stats[0]
        inv_r = lax.rsqrt(stats[1] - mean_r * mean_r + EPS)
        eighth = jnp.full((8, width), 0.125, jnp.float32)
        mean_c = dot_as(mean_r, eighth, 0, 0)
        inv_c = dot_as(inv_r, eighth, 0, 0)
        out = (accf[...] - mean_c) * inv_c * pk[5:6, :]
        out = (out * jax.nn.sigmoid(out)).astype(jnp.bfloat16)
        for place in range(n):
            for c in range(2):
                b = (place * 2 + c) * rows
                yout[c, pl.ds(place * rows, rows), :] = out[b : b + rows]
        spread(1)
        for d in range(1, n):
            stat(d).wait_send()

    for which, ref in enumerate((out_r, out_c)):
        part = ow.at[pl.ds(pl.multiple_of(which * groups + t * half, half), half)]
        pltpu.make_async_copy(ref, part, loc.at[which]).wait()
        part = ow.at[pl.ds(pl.multiple_of(which * groups + other * half, half), half)]
        remote(ref, part, o_send.at[which], o_recv.at[which], at(tp=other)).wait_recv()
    for core in range(2):
        for place in range(n):
            part = yall.at[:, pl.ds(core * groups + place * width, width)]
            pltpu.make_async_copy(part, part, a_recv.at[place, core]).wait()
    result = jnp.dot(yall[...], ow[...], preferred_element_type=jnp.float32)
    mo[...] = result.astype(jnp.bfloat16)
    cols = out_r.shape[1]
    fin_cols = pl.ds(pl.multiple_of(s * cols, cols), cols)

    def give(to_s):
        return remote(
            mo.at[pl.ds(pl.multiple_of(to_s * rows, rows), rows)], fin.at[:, fin_cols],
            f_send.at[to_s], f_recv.at[s], at(sp=to_s),
        )

    for d in range(1, n):
        give(lax.rem(s + d, n)).start()
    o_ref[0, :, fin_cols] = mo[pl.ds(pl.multiple_of(s * rows, rows), rows), :]
    for d in range(1, n):
        place = lax.rem(s + d, n)
        part_cols = pl.ds(pl.multiple_of(place * cols, cols), cols)
        remote(
            mo.at[pl.ds(0, rows)], fin.at[:, part_cols], f_send.at[place], f_recv.at[place],
            at(sp=place),
        ).wait_recv()
        o_ref[0, :, part_cols] = fin[:, part_cols]

    for core in range(2):

        @pl.when(t == core)
        def _(core=core):
            spread_wait(core)
            for e in range(1, n):
                for d in range(1, nf):
                    share(core, lax.rem(s + e, n), d).wait_send()

    for d in range(1, n):
        give(lax.rem(s + d, n)).wait_send()
    for copy in own_out:
        copy.wait_send()
    for j in range(hl):
        to_s = t * hl + j
        for core in range(2):

            @pl.when((to_s == s) & (t != core))
            def _(j=j, core=core):
                part = wbuf.at[whole(s), wcols(core)]
                remote(part, part, w_send.at[j, core], w_recv.at[s], at(tp=core)).wait_send()

            @pl.when(to_s != s)
            def _(j=j, core=core, to_s=to_s):
                part = wbuf.at[wrows(s, f), wcols(core)]
                remote(
                    part, part, w_send.at[j, core], w_recv.at[s], at(sp=to_s, tp=core)
                ).wait_send()

        @pl.when(jnp.logical_not((to_s == s) & (t == 0)))
        def _(j=j, to_s=to_s):
            remote(
                pack.at[j, pl.ds(0, PACK)], ld.at[s], l_send.at[j], l_recv.at[s],
                at(sp=to_s, tp=0),
            ).wait_send()

        @pl.when(to_s == s)
        def _(j=j):
            remote(pack.at[j], pk, p_send, p_recv, at(tp=other)).wait_send()

    for place in range(n):
        token_partner(place).wait_send()

        @pl.when((place <= s) & (s < n - 1))
        def _(place=place):
            token_right(place).wait_send()

        @pl.when((place >= s) & (s > 0))
        def _(place=place):
            token_left(place).wait_send()


def taps_half(taps):
    return taps // 2


def fused_body(
    n, nf, tokens, norm_gain, rec_query, rec_input, rec_forward, rec_backward, forget_gap,
    log_decay, rec_gain, conv_value, conv_gate, conv_kernel, conv_gain, out_rec, out_conv,
):
    hl = log_decay.shape[2]
    rows, d = tokens.shape[1:]
    total = 2 * rows * n
    taps = conv_kernel.shape[0]
    width = KD
    groups = n * width
    cols = out_rec.shape[1]

    vmem = pl.BlockSpec(memory_space=pltpu.VMEM)
    bf, f32 = jnp.bfloat16, jnp.float32
    dma = pltpu.SemaphoreType.DMA
    small = (log_decay, forget_gap, rec_gain[None], conv_gain[None], conv_kernel)
    scratch = [
        *(pltpu.VMEM(a.shape, a.dtype) for a in small),
        pltpu.VMEM(tokens.shape, bf),
        pltpu.VMEM((1, d), f32),
        pltpu.VMEM((hl, PACK + taps, width), f32),
        pltpu.VMEM((total, d), bf),
        pltpu.VMEM((d, 4 * width), bf),
        pltpu.VMEM((2 * groups, cols), bf),
        pltpu.VMEM((PACK + taps, width), f32),
        pltpu.VMEM((n, PACK, width), f32),
        pltpu.VMEM((2, total, width), f32),
        pltpu.VMEM((total, 4 * width), bf),
        pltpu.VMEM((total, width), f32),
        pltpu.VMEM((total, width), f32),
        pltpu.VMEM((total + 32, width), f32),
        pltpu.VMEM((2, total // 2, width), bf),
        pltpu.VMEM((total // 2, 2 * groups), bf),
        pltpu.VMEM((total // 2, cols), bf),
        pltpu.VMEM((rows, d), bf),
        pltpu.VMEM((n, 2, 8, total), f32),
        dma((hl, 2)), dma((n,)),
        dma((n, nf)), dma((n, nf)),
        dma((n, 2)), dma((n, 2)), dma((n,)),
        dma(()), dma(()),
        dma((hl,)), dma((n,)),
        dma((2,)), dma((2,)),
        dma((n, 2)), dma((n, 2)),
        dma((n,)), dma((n,)),
        dma((n,)), dma((n,)),
        dma((2,)), dma((7,)),
    ]
    return pl.pallas_call(
        functools.partial(fused_kernel, n, nf, hl),
        out_shape=jax.ShapeDtypeStruct((1, rows, d), bf),
        in_specs=[pl.BlockSpec(memory_space=pl.ANY)] * 15,
        out_specs=vmem,
        scratch_shapes=scratch,
        compiler_params=pltpu.CompilerParams(
            collective_id=0, has_side_effects=True, vmem_limit_bytes=60 * 1024 * 1024
        ),
    )(
        tokens, norm_gain[None], rec_query, rec_input, rec_forward, rec_backward, conv_value,
        conv_gate, *small, out_rec, out_conv,
    )


def fits(n, nf, nt, tokens, rec_query, log_decay, conv_value, conv_kernel, out_rec):
    heads = log_decay.shape[2]
    rows = tokens.shape[1] // (n * nt)
    return (
        nt == 2
        and n == heads
        and tokens.shape[0] == nf
        and rec_query.shape[1] == heads * KD
        and conv_value.shape[1] == heads * VD
        and KD == VD
        and 2 * rows == KD
        and rec_query.shape[0] % (n * nf * 16) == 0
        and conv_kernel.shape[0] // 2 <= 15
    )


def layer(mesh, *args):
    n, nf, nt = (mesh.shape[a] for a in ("sp", "fs", "tp"))
    fast = fits(n, nf, nt, args[0], args[2], args[7], args[9], args[11], args[13])
    return sharded(mesh, functools.partial(fused_body, n, nf) if fast else body)(*args)


def solution(mesh):
    return functools.partial(layer, mesh)


def sharded(mesh, body):
    return jax.shard_map(
        body,
        mesh=mesh,
        in_specs=(
            P("fs", ("sp", "tp"), None),
            P(),
            P("sp", "tp"),
            P("sp", "tp"),
            P("sp", "tp"),
            P("sp", "tp"),
            P(None, "tp"),
            P("fs", None, "tp", "sp"),
            P("tp"),
            P("sp", "tp"),
            P("sp", "tp"),
            P(None, "tp"),
            P("tp"),
            P("tp", "sp"),
            P("tp", "sp"),
        ),
        out_specs=P("fs", ("sp", "tp"), None),
        check_vma=False,
    )
```

```python
import functools

import jax
import jax.numpy as jnp
from jax import lax
from jax.experimental import pallas as pl
from jax.experimental.pallas import tpu as pltpu
from jax.sharding import PartitionSpec as P

KD = 128
VD = 128
BLOCK = 64


EPS = 1e-06
HIGH = lax.Precision.HIGHEST


def entering(x, axis, join, neutral, backward):
    count = lax.axis_size(axis)
    place = lax.axis_index(axis)
    ahead = count - 1 - place if backward else place
    gathered = jax.tree.map(
        lambda a, kind: lax.all_gather(a.astype(kind), axis), x, (jnp.bfloat16, jnp.bfloat16)
    )
    state = jax.tree.map(lambda a, e: jnp.zeros_like(a) + jnp.asarray(e, a.dtype), x, neutral)

    def one(lap, state):
        source = count - 1 - lap if backward else lap
        return join(
            state,
            jax.tree.map(
                lambda a, own: lax.dynamic_index_in_dim(a, source, 0, False).astype(own.dtype),
                gathered,
                x,
            ),
        )

    return lax.fori_loop(0, ahead, one, state)


def padded_2(cells, sides, width):
    for axis, dim in sides:
        count = lax.axis_size(axis)
        ends = count - 1
        head = lax.slice_in_dim(cells, 0, width, axis=dim)
        tail = lax.slice_in_dim(cells, cells.shape[dim] - width, cells.shape[dim], axis=dim)
        cells = jnp.concatenate(
            [
                lax.ppermute(tail, axis, [(i, (i + 1) % count) for i in range(ends)]),
                cells,
                lax.ppermute(head, axis, [((i + 1) % count, i) for i in range(ends)]),
            ],
            axis=dim,
        )
    return cells


def block_pass(queries, key_rows, value_rows, log_gate):
    heads_n, length_n, key_dim = queries.shape
    value_dim = value_rows.shape[-1]
    blocks = length_n // BLOCK

    def split_blocks(tensor):
        return tensor.reshape(heads_n, blocks, BLOCK, tensor.shape[-1]).transpose(1, 0, 2, 3)

    def join_blocks(tensor):
        return tensor.transpose(1, 0, 2, 3).reshape(heads_n, length_n, tensor.shape[-1])

    lower_mask = jnp.tril(jnp.ones((BLOCK, BLOCK), bool))

    def advance(carried, inputs):
        states, offset = carried
        query_b, key_b, value_b, gate_b = inputs
        cumulative = jnp.cumsum(gate_b, axis=1)
        query_g = query_b * jnp.exp(cumulative)
        key_g = key_b * jnp.exp(-cumulative)
        scores = jnp.einsum("htd,hsd->hts", query_g, key_g, precision=HIGH)
        scores = jnp.where(lower_mask, scores, 0.0)
        result = jnp.einsum("hts,hse->hte", scores, value_b, precision=HIGH)
        result = result + jnp.einsum("htd,hde->hte", query_g, states, precision=HIGH)
        last_g = cumulative[:, -1, :]
        weighted = key_b * jnp.exp(last_g[:, None, :] - cumulative)
        states = jnp.exp(last_g)[:, :, None] * states + jnp.einsum(
            "hsd,hse->hde", weighted, value_b, precision=HIGH
        )
        decayed = query_b * jnp.exp(offset[:, None, :] + cumulative)
        return ((states, offset + last_g), (result, decayed))

    start_state = jnp.zeros((heads_n, key_dim, value_dim), jnp.float32)
    start_offset = jnp.zeros((heads_n, key_dim), jnp.float32)
    inputs = (
        split_blocks(queries),
        split_blocks(key_rows),
        split_blocks(value_rows),
        split_blocks(log_gate),
    )
    final_pair, outputs = lax.scan(advance, (start_state, start_offset), inputs)
    return (join_blocks(outputs[0]), join_blocks(outputs[1]), final_pair[1], final_pair[0])


def chain_combine(first_part, second_part):
    return (
        first_part[0] * second_part[0],
        second_part[0][:, :, None] * first_part[1] + second_part[1],
    )


def recurrence(query_pre, input_pre, forward_pre, backward_pre, forget_gap, log_decay, rec_gain):
    heads_local = log_decay.shape[2]
    row_count = query_pre.shape[0]

    def to_heads(tensor):
        return tensor.astype(jnp.float32).reshape(row_count, heads_local, -1).transpose(1, 0, 2)

    def gate_terms(pre_act, gap_row, decay_row):
        closing = jax.nn.sigmoid(-to_heads(pre_act)) * gap_row.reshape(heads_local, 1, -1)
        return (closing, jnp.log1p(-closing) + decay_row[:, :, None])

    queries = jax.nn.silu(to_heads(query_pre)) * KD ** (-0.5)
    values = to_heads(input_pre)
    keys_fwd, gate_fwd = gate_terms(forward_pre, forget_gap[0], log_decay[0, 0])
    keys_bwd, gate_bwd = gate_terms(backward_pre, forget_gap[1], log_decay[0, 1])
    identity = (
        jnp.ones((heads_local, KD), jnp.float32),
        jnp.zeros((heads_local, KD, VD), jnp.float32),
    )
    local_fwd, decayed_fwd, offset_fwd, state_fwd = block_pass(queries, keys_fwd, values, gate_fwd)
    incoming_fwd = entering((jnp.exp(offset_fwd), state_fwd), "sp", chain_combine, identity, False)
    forward = local_fwd + jnp.einsum("htd,hde->hte", decayed_fwd, incoming_fwd[1], precision=HIGH)
    local_bwd, decayed_bwd, offset_bwd, state_bwd = block_pass(
        jnp.flip(queries, 1), jnp.flip(keys_bwd, 1), jnp.flip(values, 1), jnp.flip(gate_bwd, 1)
    )
    incoming_bwd = entering((jnp.exp(offset_bwd), state_bwd), "sp", chain_combine, identity, True)
    backward = jnp.flip(
        local_bwd + jnp.einsum("htd,hde->hte", decayed_bwd, incoming_bwd[1], precision=HIGH), 1
    )
    joined = forward + backward
    joined = joined * lax.rsqrt(jnp.mean(joined * joined, axis=-1, keepdims=True) + EPS)
    joined = joined * rec_gain.reshape(heads_local, 1, VD)
    return joined.transpose(1, 0, 2).reshape(row_count, heads_local * VD).astype(jnp.bfloat16)


def convolve(conv_pre, glu_pre, conv_kernel, conv_gain):
    gated = (conv_pre.astype(jnp.float32) * jax.nn.sigmoid(glu_pre.astype(jnp.float32))).astype(
        jnp.bfloat16
    )
    half_width = conv_kernel.shape[0] // 2
    padded = padded_2(gated, (("sp", 0),), half_width)
    convolved = lax.conv_general_dilated(
        padded.astype(jnp.float32)[None],
        conv_kernel.astype(jnp.float32)[:, None, :],
        (1,),
        "VALID",
        dimension_numbers=("NWC", "WIO", "NWC"),
        feature_group_count=gated.shape[1],
        precision=HIGH,
    )[0]
    totals = lax.psum((jnp.sum(convolved, axis=-1), jnp.sum(convolved * convolved, axis=-1)), "tp")
    full_width = convolved.shape[1] * lax.axis_size("tp")
    mean_c = (totals[0] / full_width)[:, None]
    variance = (totals[1] / full_width)[:, None] - mean_c * mean_c
    return jax.nn.silu((convolved - mean_c) * lax.rsqrt(variance + EPS) * conv_gain).astype(
        jnp.bfloat16
    )


def body(
    tokens,
    norm_gain,
    rec_query,
    rec_input,
    rec_forward,
    rec_backward,
    forget_gap,
    log_decay,
    rec_gain,
    conv_value,
    conv_gate,
    conv_kernel,
    conv_gain,
    out_rec,
    out_conv,
):
    row_values = tokens[0].astype(jnp.float32)
    normed = row_values * lax.rsqrt(jnp.mean(row_values * row_values, axis=-1, keepdims=True) + EPS)
    normed = (normed * norm_gain).astype(jnp.bfloat16)
    whole = lax.all_gather(normed, "tp", axis=0, tiled=True)
    row_count = whole.shape[0]
    pieces = (
        lax.all_gather(rec_query, "sp", axis=0, tiled=True),
        lax.all_gather(rec_input, "sp", axis=0, tiled=True),
        lax.all_gather(rec_forward, "sp", axis=0, tiled=True),
        lax.all_gather(rec_backward, "sp", axis=0, tiled=True),
        lax.all_gather(conv_value, "sp", axis=0, tiled=True),
        lax.all_gather(conv_gate, "sp", axis=0, tiled=True),
    )
    results = tuple(
        (
            jnp.dot(whole, weight_piece, preferred_element_type=jnp.float32)
            for weight_piece in pieces
        )
    )
    projected = tuple((result.astype(jnp.bfloat16) for result in results))
    rec_out = recurrence(
        projected[0], projected[1], projected[2], projected[3], forget_gap, log_decay, rec_gain
    )
    conv_out = convolve(projected[4], projected[5], conv_kernel, conv_gain)
    both_out = jnp.concatenate([rec_out, conv_out], axis=1)
    out_local = jnp.concatenate([out_rec, out_conv], axis=0)
    full_columns = lax.all_gather(out_local, "sp", axis=1, tiled=True)
    own_rows = row_count // lax.axis_size("tp")
    rows_part = lax.slice_in_dim(both_out, 0, own_rows * lax.axis_size("tp"), axis=0)
    mixed = lax.psum_scatter(
        jnp.dot(rows_part, full_columns, preferred_element_type=jnp.float32).astype(jnp.bfloat16),
        "tp",
        scatter_dimension=0,
        tiled=True,
    )
    return mixed[None]


MESH = pl.DeviceIdType.MESH
PACK = 8


def dot_as(a, b, ca, cb, precision=HIGH):
    return lax.dot_general(
        a, b, (((ca,), (cb,)), ((), ())), precision=precision, preferred_element_type=jnp.float32
    )


def dot_exact(a, b, ca, cb, split):
    parts = [a, b]
    left = parts[split]
    parts[1 - split] = parts[1 - split].astype(jnp.bfloat16)
    total = None
    for _ in range(3):
        piece = left.astype(jnp.bfloat16)
        left = left - piece.astype(jnp.float32)
        parts[split] = piece
        term = dot_as(parts[0], parts[1], ca, cb, lax.Precision.DEFAULT)
        total = term if total is None else total + term
    return total


def fused_kernel(
    n, nf, hl, tokens_in, gain_in, w0, w1, w2, w3, w4, w5, decay_in, gap_in,
    rgain_in, cgain_in, taps_in, out_r, out_c, o_ref, decay_v, gap_v, rgain_v, cgain_v, taps_v,
    tokens, gain, pack,    x, wbuf, ow, pk, ld, dec, proj, accf, accb, gp, yout, yall, mo, fin, st,
    w_send, w_recv, x_send, x_recv, t_send, t_recv, d_send, p_send, p_recv, l_send, l_recv,
    o_send, o_recv, a_send, a_recv, f_send, f_recv, s_send, s_recv, loc, ini,
):
    s = lax.axis_index("sp")
    f = lax.axis_index("fs")
    t = lax.axis_index("tp")
    other = 1 - t
    rows = tokens.shape[1]
    width = KD
    weights = (w0, w1, w2, w3, w4, w5)
    kslice = w0.shape[0]
    krows = kslice // nf
    half = out_r.shape[0]
    groups = n * width

    def at(sp=s, fs=f, tp=t):
        return {"sp": sp, "fs": fs, "tp": tp}

    def remote(src, dst, send, recv, to):
        return pltpu.make_async_remote_copy(
            src_ref=src, dst_ref=dst, send_sem=send, recv_sem=recv, device_id=to,
            device_id_type=MESH,
        )

    entry = [
        pltpu.make_async_copy(src, dst, ini.at[i])
        for i, (src, dst) in enumerate(
            (
                (tokens_in, tokens), (gain_in, gain), (decay_in, decay_v), (gap_in, gap_v),
                (rgain_in, rgain_v), (cgain_in, cgain_v), (taps_in, taps_v),
            )
        )
    ]
    for copy in entry:
        copy.start()

    barrier = pltpu.get_barrier_semaphore()
    for d in range(n):
        for c in range(2):
            if d or c:
                pl.semaphore_signal(
                    barrier, inc=1, device_id=at(sp=lax.rem(s + d, n), tp=lax.rem(t + c, 2)),
                    device_id_type=MESH,
                )
    for d in range(1, nf):
        pl.semaphore_signal(
            barrier, inc=1, device_id=at(fs=lax.rem(f + d, nf)), device_id_type=MESH
        )
    pl.semaphore_wait(barrier, 2 * n - 1 + nf - 1)

    def wrows(place, quarter):
        return pl.ds(pl.multiple_of(place * kslice + quarter * krows, krows), krows)

    def wcols(core):
        return pl.ds(0, (4 - 2 * core) * width)

    def whole(place):
        return pl.ds(pl.multiple_of(place * kslice, kslice), kslice)

    mine = pl.ds(pl.multiple_of(f * krows, krows), krows)
    for j in range(hl):
        to_s = t * hl + j
        cols = pl.ds(j * width, width)
        for core in range(2):
            for at_m, m in enumerate((0, 1, 2, 3) if core == 0 else (4, 5)):
                at_cols = pl.ds(at_m * width, width)
                src = weights[m].at[:, cols]
                dst = wbuf.at[whole(s), at_cols]

                @pl.when((to_s == s) & (t == core))
                def _(src=src, dst=dst):
                    pltpu.make_async_copy(src, dst, w_recv.at[s]).start()

                @pl.when((to_s == s) & (t != core))
                def _(src=src, dst=dst, core=core, j=j):
                    remote(src, dst, w_send.at[j, core], w_recv.at[s], at(tp=core)).start()

                @pl.when(to_s != s)
                def _(m=m, cols=cols, at_cols=at_cols, core=core, to_s=to_s, j=j):
                    remote(
                        weights[m].at[mine, cols], wbuf.at[wrows(s, f), at_cols],
                        w_send.at[j, core], w_recv.at[s], at(sp=to_s, tp=core),
                    ).start()

    for copy in entry[2:]:
        copy.wait()
    taps_n = taps_v.shape[0]
    for j in range(hl):
        cols = slice(j * width, (j + 1) * width)
        pack[j, 0:2, :] = decay_v[0, :, j, :]
        pack[j, 2:4, :] = gap_v[:, cols]
        pack[j, 4:5, :] = rgain_v[:, cols]
        pack[j, 5:6, :] = cgain_v[:, cols]
        pack[j, 6:PACK, :] = jnp.zeros((PACK - 6, width), jnp.float32)
        pack[j, PACK : PACK + taps_n, :] = taps_v[:, cols].astype(jnp.float32)
    entry[0].wait()
    entry[1].wait()
    values = tokens[0].astype(jnp.float32)
    normed = values * lax.rsqrt(jnp.mean(values * values, axis=-1, keepdims=True) + EPS)

    def slot(place, core):
        return pl.ds(pl.multiple_of(place * 2 * rows + core * rows, rows), rows)

    x[slot(s, t), :] = (normed * gain[...]).astype(jnp.bfloat16)

    def token(place, core, send, to):
        part = x.at[slot(place, core)]
        return remote(part, part, send, t_recv.at[place, core], to)

    def token_right(place):
        return token(place, t, t_send.at[place, 0], at(sp=lax.rem(s + 1, n)))

    def token_left(place):
        return token(place, t, t_send.at[place, 1], at(sp=lax.rem(s + n - 1, n)))

    def token_partner(place):
        return token(place, t, d_send.at[place], at(tp=other))

    @pl.when(s < n - 1)
    def _():
        token_right(s).start()

    @pl.when(s > 0)
    def _():
        token_left(s).start()

    token_partner(s).start()

    for j in range(hl):
        to_s = t * hl + j
        here0 = (to_s == s) & (t == 0)
        src = pack.at[j, pl.ds(0, PACK)]

        @pl.when(here0)
        def _(src=src):
            pltpu.make_async_copy(src, ld.at[s], l_recv.at[s]).start()

        @pl.when(jnp.logical_not(here0))
        def _(src=src, j=j, to_s=to_s):
            remote(src, ld.at[s], l_send.at[j], l_recv.at[s], at(sp=to_s, tp=0)).start()

        @pl.when(to_s == s)
        def _(j=j):
            pltpu.make_async_copy(pack.at[j], pk, p_recv).start()
            remote(pack.at[j], pk, p_send, p_recv, at(tp=other)).start()

    own_out = []
    for which, ref in enumerate((out_r, out_c)):
        part = ow.at[pl.ds(pl.multiple_of(which * groups + t * half, half), half)]
        own_out.append(remote(ref, part, o_send.at[which], o_recv.at[which], at(tp=other)))
        own_out[-1].start()
        pltpu.make_async_copy(ref, part, loc.at[which]).start()

    def share(core, place, d):
        part = wbuf.at[wrows(place, f), wcols(core)]
        return remote(
            part, part, x_send.at[place, d], x_recv.at[place, f], at(fs=lax.rem(f + d, nf))
        )

    for core in range(2):

        @pl.when(t == core)
        def _(core=core):
            for e in range(1, n):
                place = lax.rem(s + e, n)
                part = wbuf.at[wrows(place, f), wcols(core)]
                pltpu.make_async_copy(part, part, w_recv.at[place]).wait()
                for d in range(1, nf):
                    share(core, place, d).start()

    for d in range(1, n):

        @pl.when(s >= d)
        def _(d=d):
            place = s - d
            token_right(place).wait_recv()
            token_partner(place).start()

            @pl.when(s < n - 1)
            def _():
                token_right(place).start()

        @pl.when(s + d < n)
        def _(d=d):
            place = s + d
            token_left(place).wait_recv()
            token_partner(place).start()

            @pl.when(s > 0)
            def _():
                token_left(place).start()

    for place in range(n):
        part = x.at[slot(place, other)]
        remote(part, part, d_send.at[place], t_recv.at[place, other], at(tp=other)).wait_recv()
    for core in range(2):

        @pl.when(t == core)
        def _(core=core):
            part = wbuf.at[whole(s), wcols(core)]
            pltpu.make_async_copy(part, part, w_recv.at[s]).wait()
            for e in range(1, n):
                place = lax.rem(s + e, n)
                for d in range(1, nf):
                    quarter = lax.rem(f + d, nf)
                    part = wbuf.at[wrows(place, quarter), wcols(core)]
                    remote(
                        part, part, x_send.at[place, d], x_recv.at[place, quarter], at(fs=quarter)
                    ).wait_recv()

    pltpu.make_async_copy(pk, pk, p_recv).wait()

    total = x.shape[0]
    chunk = min(256, total)

    def project(core):
        @pl.loop(0, total // chunk)
        def _(i):
            at_rows = pl.ds(pl.multiple_of(i * chunk, chunk), chunk)
            proj[at_rows, wcols(core)] = jnp.dot(
                x[at_rows, :], wbuf[:, wcols(core)], preferred_element_type=jnp.float32
            ).astype(jnp.bfloat16)

    def send_all(core, to_s, to_t):
        dst = yall.at[:, pl.ds(pl.multiple_of(core * groups + s * width, width), width)]
        return remote(
            yout.at[to_t], dst, a_send.at[to_s, to_t], a_recv.at[s, core], at(sp=to_s, tp=to_t)
        )

    def spread(core):
        for d in range(n):
            for c in range(2):
                if d or c:
                    send_all(core, lax.rem(s + n - d, n), (core + c) % 2).start()
        dst = yall.at[:, pl.ds(pl.multiple_of(core * groups + s * width, width), width)]
        pltpu.make_async_copy(yout.at[core], dst, a_recv.at[s, core]).start()

    def spread_wait(core):
        for d in range(n):
            for c in range(2):
                if d or c:
                    send_all(core, lax.rem(s + n - d, n), (core + c) % 2).wait_send()

    @pl.when(t == 0)
    def _():
        project(0)
        for place in range(n):
            pltpu.make_async_copy(ld.at[place], ld.at[place], l_recv.at[place]).wait()
        pick = lax.broadcasted_iota(jnp.int32, (PACK, width), 0)
        span = 2 * rows
        for place in range(n):
            for d in range(2):
                dec[d, pl.ds(place * span, span), :] = dot_as(
                    ld[place], (pick == d).astype(jnp.float32), 0, 0
                )
        row_i = lax.broadcasted_iota(jnp.int32, (BLOCK, BLOCK), 0)
        col_i = lax.broadcasted_iota(jnp.int32, (BLOCK, BLOCK), 1)
        masks = (row_i >= col_i, row_i <= col_i)
        blocks = total // BLOCK

        def one(d, p, state):
            at_rows = pl.ds(pl.multiple_of(p * BLOCK, BLOCK), BLOCK)
            qp = proj[at_rows, 0:width].astype(jnp.float32)
            query = qp * jax.nn.sigmoid(qp) * width ** (-0.5)
            value = proj[at_rows, width : 2 * width].astype(jnp.float32)
            pre = proj[at_rows, (2 + d) * width : (3 + d) * width].astype(jnp.float32)
            keys = pk[2 + d : 3 + d, :] * jax.nn.sigmoid(-pre)
            gate = jnp.log1p(-keys) + dec[d, at_rows, :]
            cum = dot_exact(masks[d].astype(jnp.float32), gate, 1, 0, 1)
            query_g = query * jnp.exp(cum)
            key_g = keys * jnp.exp(-cum)
            scores = jnp.where(masks[d], dot_as(query_g, key_g, 1, 1), 0.0)
            result = dot_as(scores, value, 1, 0) + dot_as(query_g, state, 1, 1)
            last = cum[BLOCK - 1 : BLOCK, :] if d == 0 else cum[0:1, :]
            weighted = keys * jnp.exp(last - cum)
            state = state * jnp.exp(last) + dot_as(value, weighted, 0, 0)
            (accf, accb)[d][at_rows, :] = result
            return state

        def step(i, states):
            return one(0, i, states[0]), one(1, blocks - 1 - i, states[1])

        zero = jnp.zeros((width, width), jnp.float32)
        lax.fori_loop(0, blocks, step, (zero, zero))
        for place in range(n):
            for c in range(2):
                at_rows = pl.ds((place * 2 + c) * rows, rows)
                joined = accf[at_rows, :] + accb[at_rows, :]
                joined = joined * lax.rsqrt(
                    jnp.mean(joined * joined, axis=-1, keepdims=True) + EPS
                )
                yout[c, pl.ds(place * rows, rows), :] = (joined * pk[4:5, :]).astype(jnp.bfloat16)
        spread(0)

    @pl.when(t == 1)
    def _():
        project(1)
        taps = pk.shape[0] - PACK
        pad = 16
        gp[0:pad, :] = jnp.zeros((pad, width), jnp.float32)
        gp[pad + total : 2 * pad + total, :] = jnp.zeros((pad, width), jnp.float32)
        value = proj[:, 0:width].astype(jnp.float32)
        gate = proj[:, width : 2 * width].astype(jnp.float32)
        gp[pad : pad + total, :] = (
            (value * jax.nn.sigmoid(gate)).astype(jnp.bfloat16).astype(jnp.float32)
        )
        first = pad - taps_half(taps)

        for b in range(total // rows):
            acc = jnp.zeros((rows, width), jnp.float32)
            for j in range(taps):
                acc = acc + pk[PACK + j : PACK + j + 1, :] * gp[pl.ds(b * rows + first + j, rows), :]
            accf[pl.ds(b * rows, rows), :] = acc
        conv = accf[...]
        ones = jnp.ones((8, width), jnp.float32)
        st[s, 0] = dot_exact(ones, conv, 1, 1, 1)
        st[s, 1] = dot_exact(ones, conv * conv, 1, 1, 1)

        def stat(d):
            return remote(
                st.at[s], st.at[s], s_send.at[d], s_recv.at[s], at(sp=lax.rem(s + d, n))
            )

        for d in range(1, n):
            stat(d).start()
        for d in range(1, n):
            place = lax.rem(s + d, n)
            remote(st.at[place], st.at[place], s_send.at[d], s_recv.at[place], at(sp=place)).wait_recv()
        stats = st[0]
        for place in range(1, n):
            stats = stats + st[place]
        stats = stats / groups
        mean_r = stats[0]
        inv_r = lax.rsqrt(stats[1] - mean_r * mean_r + EPS)
        eighth = jnp.full((8, width), 0.125, jnp.float32)
        mean_c = dot_exact(mean_r, eighth, 0, 0, 0)
        inv_c = dot_exact(inv_r, eighth, 0, 0, 0)
        out = (accf[...] - mean_c) * inv_c * pk[5:6, :]
        out = (out * jax.nn.sigmoid(out)).astype(jnp.bfloat16)
        for place in range(n):
            for c in range(2):
                b = (place * 2 + c) * rows
                yout[c, pl.ds(place * rows, rows), :] = out[b : b + rows]
        spread(1)
        for d in range(1, n):
            stat(d).wait_send()

    for which, ref in enumerate((out_r, out_c)):
        part = ow.at[pl.ds(pl.multiple_of(which * groups + t * half, half), half)]
        pltpu.make_async_copy(ref, part, loc.at[which]).wait()
        part = ow.at[pl.ds(pl.multiple_of(which * groups + other * half, half), half)]
        remote(ref, part, o_send.at[which], o_recv.at[which], at(tp=other)).wait_recv()
    for core in range(2):
        for place in range(n):
            part = yall.at[:, pl.ds(core * groups + place * width, width)]
            pltpu.make_async_copy(part, part, a_recv.at[place, core]).wait()
    result = jnp.dot(yall[...], ow[...], preferred_element_type=jnp.float32)
    mo[...] = result.astype(jnp.bfloat16)
    cols = out_r.shape[1]
    fin_cols = pl.ds(pl.multiple_of(s * cols, cols), cols)

    def give(to_s):
        return remote(
            mo.at[pl.ds(pl.multiple_of(to_s * rows, rows), rows)], fin.at[:, fin_cols],
            f_send.at[to_s], f_recv.at[s], at(sp=to_s),
        )

    for d in range(1, n):
        give(lax.rem(s + d, n)).start()
    o_ref[0, :, fin_cols] = mo[pl.ds(pl.multiple_of(s * rows, rows), rows), :]
    for d in range(1, n):
        place = lax.rem(s + d, n)
        part_cols = pl.ds(pl.multiple_of(place * cols, cols), cols)
        remote(
            mo.at[pl.ds(0, rows)], fin.at[:, part_cols], f_send.at[place], f_recv.at[place],
            at(sp=place),
        ).wait_recv()
        o_ref[0, :, part_cols] = fin[:, part_cols]

    for core in range(2):

        @pl.when(t == core)
        def _(core=core):
            spread_wait(core)
            for e in range(1, n):
                for d in range(1, nf):
                    share(core, lax.rem(s + e, n), d).wait_send()

    for d in range(1, n):
        give(lax.rem(s + d, n)).wait_send()
    for copy in own_out:
        copy.wait_send()
    for j in range(hl):
        to_s = t * hl + j
        for core in range(2):

            @pl.when((to_s == s) & (t != core))
            def _(j=j, core=core):
                part = wbuf.at[whole(s), wcols(core)]
                remote(part, part, w_send.at[j, core], w_recv.at[s], at(tp=core)).wait_send()

            @pl.when(to_s != s)
            def _(j=j, core=core, to_s=to_s):
                part = wbuf.at[wrows(s, f), wcols(core)]
                remote(
                    part, part, w_send.at[j, core], w_recv.at[s], at(sp=to_s, tp=core)
                ).wait_send()

        @pl.when(jnp.logical_not((to_s == s) & (t == 0)))
        def _(j=j, to_s=to_s):
            remote(
                pack.at[j, pl.ds(0, PACK)], ld.at[s], l_send.at[j], l_recv.at[s],
                at(sp=to_s, tp=0),
            ).wait_send()

        @pl.when(to_s == s)
        def _(j=j):
            remote(pack.at[j], pk, p_send, p_recv, at(tp=other)).wait_send()

    for place in range(n):
        token_partner(place).wait_send()

        @pl.when((place <= s) & (s < n - 1))
        def _(place=place):
            token_right(place).wait_send()

        @pl.when((place >= s) & (s > 0))
        def _(place=place):
            token_left(place).wait_send()


def taps_half(taps):
    return taps // 2


def fused_body(
    n, nf, tokens, norm_gain, rec_query, rec_input, rec_forward, rec_backward, forget_gap,
    log_decay, rec_gain, conv_value, conv_gate, conv_kernel, conv_gain, out_rec, out_conv,
):
    hl = log_decay.shape[2]
    rows, d = tokens.shape[1:]
    total = 2 * rows * n
    taps = conv_kernel.shape[0]
    width = KD
    groups = n * width
    cols = out_rec.shape[1]

    vmem = pl.BlockSpec(memory_space=pltpu.VMEM)
    bf, f32 = jnp.bfloat16, jnp.float32
    dma = pltpu.SemaphoreType.DMA
    small = (log_decay, forget_gap, rec_gain[None], conv_gain[None], conv_kernel)
    scratch = [
        *(pltpu.VMEM(a.shape, a.dtype) for a in small),
        pltpu.VMEM(tokens.shape, bf),
        pltpu.VMEM((1, d), f32),
        pltpu.VMEM((hl, PACK + taps, width), f32),
        pltpu.VMEM((total, d), bf),
        pltpu.VMEM((d, 4 * width), bf),
        pltpu.VMEM((2 * groups, cols), bf),
        pltpu.VMEM((PACK + taps, width), f32),
        pltpu.VMEM((n, PACK, width), f32),
        pltpu.VMEM((2, total, width), f32),
        pltpu.VMEM((total, 4 * width), bf),
        pltpu.VMEM((total, width), f32),
        pltpu.VMEM((total, width), f32),
        pltpu.VMEM((total + 32, width), f32),
        pltpu.VMEM((2, total // 2, width), bf),
        pltpu.VMEM((total // 2, 2 * groups), bf),
        pltpu.VMEM((total // 2, cols), bf),
        pltpu.VMEM((rows, d), bf),
        pltpu.VMEM((n, 2, 8, total), f32),
        dma((hl, 2)), dma((n,)),
        dma((n, nf)), dma((n, nf)),
        dma((n, 2)), dma((n, 2)), dma((n,)),
        dma(()), dma(()),
        dma((hl,)), dma((n,)),
        dma((2,)), dma((2,)),
        dma((n, 2)), dma((n, 2)),
        dma((n,)), dma((n,)),
        dma((n,)), dma((n,)),
        dma((2,)), dma((7,)),
    ]
    return pl.pallas_call(
        functools.partial(fused_kernel, n, nf, hl),
        out_shape=jax.ShapeDtypeStruct((1, rows, d), bf),
        in_specs=[pl.BlockSpec(memory_space=pl.ANY)] * 15,
        out_specs=vmem,
        scratch_shapes=scratch,
        compiler_params=pltpu.CompilerParams(
            collective_id=0, has_side_effects=True, vmem_limit_bytes=60 * 1024 * 1024
        ),
    )(
        tokens, norm_gain[None], rec_query, rec_input, rec_forward, rec_backward, conv_value,
        conv_gate, *small, out_rec, out_conv,
    )


def fits(n, nf, nt, tokens, rec_query, log_decay, conv_value, conv_kernel, out_rec):
    heads = log_decay.shape[2]
    rows = tokens.shape[1] // (n * nt)
    return (
        nt == 2
        and n == heads
        and tokens.shape[0] == nf
        and rec_query.shape[1] == heads * KD
        and conv_value.shape[1] == heads * VD
        and KD == VD
        and 2 * rows == KD
        and rec_query.shape[0] % (n * nf * 16) == 0
        and conv_kernel.shape[0] // 2 <= 15
    )


def layer(mesh, *args):
    n, nf, nt = (mesh.shape[a] for a in ("sp", "fs", "tp"))
    fast = fits(n, nf, nt, args[0], args[2], args[7], args[9], args[11], args[13])
    return sharded(mesh, functools.partial(fused_body, n, nf) if fast else body)(*args)


def solution(mesh):
    return functools.partial(layer, mesh)


def sharded(mesh, body):
    return jax.shard_map(
        body,
        mesh=mesh,
        in_specs=(
            P("fs", ("sp", "tp"), None),
            P(),
            P("sp", "tp"),
            P("sp", "tp"),
            P("sp", "tp"),
            P("sp", "tp"),
            P(None, "tp"),
            P("fs", None, "tp", "sp"),
            P("tp"),
            P("sp", "tp"),
            P("sp", "tp"),
            P(None, "tp"),
            P("tp"),
            P("tp", "sp"),
            P("tp", "sp"),
        ),
        out_specs=P("fs", ("sp", "tp"), None),
        check_vma=False,
    )
```
